256 devices in a mesh: ep: 64 (over z, y, core), tp: 4 (over x).
Axes of the slice: x: 4, y: 4, z: 8, core: 2. Of those that a mesh axis runs over, the one named last changes fastest.
Arguments:
- mixer_input: bfloat16 [32768, 2048], P('ep'), may hold values from -6 to 6
- mixer_gain: bfloat16 [2048], replicated, may hold values from 0.099609375 to 1.8984375
- pool_in: bfloat16 [2048, 1024], P(None, 'tp'), may hold values from -0.125 to 0.125
- pool_map: bfloat16 [4, 256, 256], P('tp'), may hold values from -0.375 to 0.375
- pool_scale: bfloat16 [1024], P('tp'), may hold values from 0.099609375 to 1.8984375
- pool_out: bfloat16 [1024, 2048], P('tp'), may hold values from -0.1875 to 0.1875
- expert_input: bfloat16 [24576, 2048], P('ep'), may hold values from -6 to 6
- expert_gain: bfloat16 [2048], replicated, may hold values from 0.099609375 to 1.8984375
- group_router: bfloat16 [2048, 4], replicated, may hold values from -0.125 to 0.125
- expert_router: bfloat16 [2048, 64], replicated, may hold values from -0.125 to 0.125
- routes: int32 [24576, 2], P('ep'), may hold values from 0 to 63, all different within a row; in each aligned block of 96 rows (0 to 95, 96 to 191, ...) at most 6 rows name the same one
- gate_weight: bfloat16 [64, 2048, 1024], P('ep', None, 'tp'), may hold values from -0.125 to 0.125
- up_weight: bfloat16 [64, 2048, 1024], P('ep', None, 'tp'), may hold values from -0.125 to 0.125
- down_weight: bfloat16 [64, 1024, 2048], P('ep', 'tp'), may hold values from -0.1875 to 0.1875
Outputs:
- mixer_output: bfloat16 [32768, 2048], P(('ep', 'tp'))
- expert_output: bfloat16 [24576, 2048], P(('ep', 'tp'))
The draws below stay inside these ranges and needn't reach their ends.
Inputs may be any that keep to these rules, and one draw needn't show every extreme that they name: `routes`: each row names two different experts. In each aligned block of 96 rows no expert is named more than 6 times, a bound that some block reaches.
All inputs are finite; a program needn't handle non-finite values.
Results may differ from the reference program's by a relative error of at most 0.01.
Values may be sent and summed in bfloat16 or wider, within the bound.
A program may use at most 64 MiB of HBM per device.

```python
import math
import jax
import jax.numpy as jnp
import numpy as np
from jax import lax

D = 2048
MIX_A = 1024
POOL_GROUPS = 4
POOL_CH = 256
RIM = 15
HID = 1024
EXPERT_GROUPS = 4
EXPERTS = 64
TOK_A = 32768
TB_DEV = 96
TOK_B = 24576
CAPQ = 6
N_TP = 4


def levels(stream_key, extent, shards, least, largest):
    loudness, own = 1.0, jax.random.fold_in(stream_key, 6)
    for dim, parts in shards:
        draws = jnp.exp(jax.random.uniform(jax.random.fold_in(own, dim), (parts,), jnp.float32, least / len(shards), largest / len(shards)))
        loudness = loudness * jnp.repeat(draws, extent[dim] // parts).reshape([-1 if axis == dim else 1 for axis in range(len(extent))])
    return loudness


def shared_out(own_key, own, number, rows, number_of, top, bound, lean):
    order = jax.random.permutation(own_key, number_of)
    crowded, usual = portions_of(number_of, rows * top, bound, lean, True), portions_of(number_of, rows * top, bound, lean, False)
    places = jnp.arange(number_of)

    def named(lengths, turn):
        used = int((lengths > 0).sum())
        fixed = max(1, used // 4)
        shifted = fixed + (places - fixed + turn * (used - fixed)) % max(1, number_of - fixed)
        return jnp.zeros((number_of,), jnp.int32).at[order[jnp.where(places < fixed, places, shifted)]].set(jnp.asarray(lengths, jnp.int32))

    lengths = jnp.where(number % 4 == 0, named(crowded, number // 4), named(usual, number - number // 4 - 1))
    mixed = jax.random.permutation(jax.random.fold_in(own, 3), number_of)
    giver, sink = mixed[0:number_of // 2 * 2:2], mixed[1:number_of // 2 * 2:2]
    room = jnp.minimum(lengths[giver] - 1, bound - lengths[sink]) // 2
    room = jnp.where((giver == order[0]) | (sink == order[0]) | (lengths[sink] == 0), 0, jnp.maximum(room, 0))
    shifted = jax.random.randint(jax.random.fold_in(own, 4), (number_of // 2,), 0, 1 << 20) % (room + 1)
    lengths = lengths.at[giver].add(-shifted).at[sink].add(shifted)
    labels = jnp.searchsorted(jnp.cumsum(lengths), jnp.arange(rows * top), side="right").astype(jnp.int32)
    grid = labels.reshape(top, rows).T
    grid = grid[jax.random.permutation(jax.random.fold_in(own, 1), rows)]
    turn = jax.random.randint(jax.random.fold_in(own, 2), (rows, 1), 0, top)
    return jnp.take_along_axis(grid, (jnp.arange(top)[None, :] + turn) % top, axis=1)


def portions_of(number_of, total, most, lean, full):
    loads = [(1 << 20) // math.isqrt(grade ** lean) + 1 for grade in range(1, number_of + 1)]
    largest = most if full else min(most, max(-(-total // number_of), total * loads[0] // sum(loads)))
    least = 1 if total - largest >= number_of - 1 else 0
    holding, spare = [largest] + [least] * (number_of - 1), total - largest - least * (number_of - 1)
    while spare > 0:
        movable = [i for i in range(1, number_of) if holding[i] < largest] or [i for i in range(1, number_of) if holding[i] < most]
        mass, budget = sum([loads[i] for i in movable]), spare
        for i in movable:
            more = min(most - holding[i], max(1, budget * loads[i] // mass), spare)
            holding[i] = holding[i] + more
            spare = spare - more
    return np.array(holding)


def normal_values(key, extent, spread, most, shards=(), held_as=jnp.bfloat16):
    entries = spread * jax.random.normal(key, extent, jnp.float32)
    if shards:
        entries = entries * levels(key, extent, shards, -0.22, 0.18)
    return jnp.clip(entries, -most, most).astype(held_as)


def setup_inputs(seed: int = 0) -> dict:
    key_of = jax.random.split(jax.random.key(seed), 15)
    mixer_input = normal_values(key_of[0], (TOK_A, D), 1.0, 6.0, ((0, 64),))
    mixer_gain = jnp.clip(1.0 + 0.18 * jax.random.normal(key_of[1], (D,), jnp.float32), 0.099609375, 1.8984375).astype(jnp.bfloat16)
    pool_in = normal_values(key_of[2], (D, MIX_A), D ** -0.5, 0.125, ((1, 4),))
    pool_map = normal_values(key_of[3], (POOL_GROUPS, POOL_CH, POOL_CH), POOL_CH ** -0.5, 0.375, ((0, 4),))
    pool_scale = jnp.clip(1.0 + 0.18 * jax.random.normal(key_of[4], (MIX_A,), jnp.float32), 0.099609375, 1.8984375).astype(jnp.bfloat16)
    pool_out = normal_values(key_of[5], (MIX_A, D), MIX_A ** -0.5, 0.1875, ((0, 4),))
    expert_input = normal_values(key_of[6], (TOK_B, D), 1.0, 6.0, ((0, 64),))
    expert_gain = jnp.clip(1.0 + 0.18 * jax.random.normal(key_of[7], (D,), jnp.float32), 0.099609375, 1.8984375).astype(jnp.bfloat16)
    group_router = normal_values(key_of[8], (D, EXPERT_GROUPS), D ** -0.5, 0.125)
    expert_router = normal_values(key_of[9], (D, EXPERTS), D ** -0.5, 0.125)
    routes_keys = jax.random.split(jax.random.fold_in(key_of[10], 1), TOK_B // TB_DEV)
    routes_turns = jax.random.permutation(jax.random.fold_in(key_of[10], 3), TOK_B // TB_DEV)
    routes = jax.vmap(lambda own, number: shared_out(jax.random.fold_in(key_of[10], 2), own, number, TB_DEV, EXPERTS, 2, CAPQ, 2))(routes_keys, routes_turns).reshape((TOK_B, 2))
    gate_weight = normal_values(key_of[11], (EXPERTS, D, HID), D ** -0.5, 0.125, ((0, 64), (2, 4)))
    up_weight = normal_values(key_of[12], (EXPERTS, D, HID), D ** -0.5, 0.125, ((0, 64), (2, 4)))
    down_weight = normal_values(key_of[13], (EXPERTS, HID, D), HID ** -0.5, 0.1875, ((0, 64), (1, 4)))
    return {"mixer_input": mixer_input, "mixer_gain": mixer_gain, "pool_in": pool_in, "pool_map": pool_map, "pool_scale": pool_scale, "pool_out": pool_out, "expert_input": expert_input, "expert_gain": expert_gain, "group_router": group_router, "expert_router": expert_router, "routes": routes, "gate_weight": gate_weight, "up_weight": up_weight, "down_weight": down_weight}


EPS = 1e-06
block_rows = 128

def norm_rows(values, gain):
    floats = values.astype(jnp.float32)
    scale = lax.rsqrt(lax.optimization_barrier(jnp.mean(floats * floats, axis=-1, keepdims=True)) + EPS)
    return (floats * scale * gain.astype(jnp.float32)).astype(jnp.bfloat16)

def route_weights(rows, group_router, expert_router, route_rows):
    group_logits = jnp.dot(rows, group_router, preferred_element_type=jnp.float32)
    expert_logits = jnp.dot(rows, expert_router, preferred_element_type=jnp.float32)
    groups = group_logits.shape[1]
    experts = expert_logits.shape[1]
    member = (jnp.arange(experts, dtype=jnp.int32)[:, None] // (experts // groups) == jnp.arange(groups, dtype=jnp.int32)[None, :]).astype(jnp.float32)
    group_exp = jnp.exp(group_logits)
    group_prob = group_exp / lax.optimization_barrier(jnp.sum(group_exp, axis=1, keepdims=True))
    expert_exp = jnp.exp(expert_logits)
    within = jnp.dot(expert_exp, member, precision=lax.Precision.HIGHEST)
    prob = expert_exp * jnp.dot(group_prob / within, member.T, precision=lax.Precision.HIGHEST)
    chosen = (route_rows[:, :, None] == jnp.arange(experts, dtype=jnp.int32)[None, None, :]).astype(jnp.float32)
    picked = lax.optimization_barrier(jnp.sum(chosen * prob[:, None, :], axis=2))
    return picked / lax.optimization_barrier(jnp.sum(picked, axis=1, keepdims=True))

def reference(mixer_input, mixer_gain, pool_in, pool_map, pool_scale, pool_out, expert_input, expert_gain, group_router, expert_router, routes, gate_weight, up_weight, down_weight):
    normed = norm_rows(mixer_input, mixer_gain)
    pooled_in = jnp.dot(normed, pool_in, preferred_element_type=jnp.float32).astype(jnp.bfloat16)
    tokens = pooled_in.shape[0]
    floats = pooled_in.astype(jnp.float32).reshape(tokens, POOL_GROUPS, POOL_CH)
    padded = jnp.concatenate([jnp.zeros((RIM, POOL_GROUPS, POOL_CH), jnp.float32), floats], axis=0)
    position = jnp.arange(tokens, dtype=jnp.int32)
    group_list = []
    for group in range(POOL_GROUPS):
        window = 2 ** (group + 1)
        window_sum = jnp.zeros((tokens, POOL_CH), jnp.float32)
        for offset in range(window):
            window_sum = window_sum + padded[RIM - offset:RIM - offset + tokens, group]
        counts = jnp.minimum(position + 1, window).astype(jnp.float32)
        group_list.append(window_sum / counts[:, None] - floats[:, group])
    pooled = jnp.stack(group_list, axis=1).astype(jnp.bfloat16)
    mapped = jnp.einsum('tgc,gce->tge', pooled.astype(jnp.float32), pool_map.astype(jnp.float32))
    mixed = (mapped.reshape(tokens, MIX_A) * pool_scale.astype(jnp.float32)).astype(jnp.bfloat16)
    quarter = MIX_A // N_TP
    mixer_sum = jnp.zeros((tokens, D), jnp.float32)
    for part in range(N_TP):
        partial_value = jnp.dot(mixed[:, part * quarter:(part + 1) * quarter], pool_out[part * quarter:(part + 1) * quarter], preferred_element_type=jnp.float32).astype(jnp.bfloat16)
        partial_value = lax.optimization_barrier(partial_value)
        mixer_sum = mixer_sum + partial_value.astype(jnp.float32)
    mixer_output = mixer_sum.astype(jnp.bfloat16)
    normed_exp = norm_rows(expert_input, expert_gain)
    weights = route_weights(normed_exp, group_router, expert_router, routes)
    tokens_b = normed_exp.shape[0]
    flat = routes.reshape(-1).astype(jnp.int32)
    assigned = flat.shape[0]
    owner = (jnp.arange(assigned, dtype=jnp.int32) // 2).astype(jnp.int32)
    order = jnp.argsort(flat, stable=True).astype(jnp.int32)
    sorted_expert = flat[order]
    sorted_owner = owner[order]
    counts_all = lax.optimization_barrier(jnp.sum((flat[:, None] == jnp.arange(EXPERTS, dtype=jnp.int32)[None, :]).astype(jnp.int32), axis=0))
    starts = (jnp.cumsum(counts_all) - counts_all).astype(jnp.int32)
    padded_counts = (counts_all + block_rows - 1) // block_rows * block_rows
    pad_starts = (jnp.cumsum(padded_counts) - padded_counts).astype(jnp.int32)
    pad_ends = pad_starts + padded_counts
    dest = (pad_starts[sorted_expert] + jnp.arange(assigned, dtype=jnp.int32) - starts[sorted_expert]).astype(jnp.int32)
    blocks = (assigned + EXPERTS * (block_rows - 1) + block_rows - 1) // block_rows
    buffer = jnp.zeros((blocks * block_rows, D), jnp.bfloat16).at[dest].set(normed_exp[sorted_owner])
    block_start = jnp.arange(blocks, dtype=jnp.int32) * block_rows
    block_expert = jnp.clip(lax.optimization_barrier(jnp.sum((pad_ends[None, :] <= block_start[:, None]).astype(jnp.int32), axis=1)), 0, EXPERTS - 1).astype(jnp.int32)
    hid_part = HID // N_TP

    def expert_block(pair):
        rows_here, expert = pair
        gate = jnp.dot(rows_here, gate_weight[expert], preferred_element_type=jnp.float32)
        upward = jnp.dot(rows_here, up_weight[expert], preferred_element_type=jnp.float32)
        hidden = (jax.nn.silu(gate) * upward).astype(jnp.bfloat16)
        result = jnp.zeros((block_rows, D), jnp.float32)
        for part in range(N_TP):
            partial_value = jnp.dot(hidden[:, part * hid_part:(part + 1) * hid_part], down_weight[expert, part * hid_part:(part + 1) * hid_part], preferred_element_type=jnp.float32).astype(jnp.bfloat16)
            partial_value = lax.optimization_barrier(partial_value)
            result = result + partial_value.astype(jnp.float32)
        return result.astype(jnp.bfloat16)
    results = lax.map(expert_block, (buffer.reshape(blocks, block_rows, D), block_expert)).reshape(-1, D)
    per_copy = results[dest].astype(jnp.float32)
    copy_weight = weights.reshape(-1)[order]
    expert_sum = jnp.zeros((tokens_b, D), jnp.float32).at[sorted_owner].add(per_copy * copy_weight[:, None])
    return (mixer_output, expert_sum.astype(jnp.bfloat16))
```

```python
import functools

import jax
import jax.numpy as jnp
from jax import lax
from jax.experimental import pallas as pl
from jax.experimental.pallas import tpu as pltpu
from jax.sharding import PartitionSpec as P

EPS = 1e-06
RIM = 16
CHUNKS = 4
MESH = pl.DeviceIdType.MESH
F32 = jnp.float32
BF16 = jnp.bfloat16


def iota(shape, dim):
    return lax.broadcasted_iota(jnp.int32, shape, dim)


def over(value, divisor):
    return (value * (-(-65536 // divisor))) >> 16


def ones_where(mask):
    return jnp.where(mask, 1.0, 0.0).astype(BF16)


def dot(a, b):
    return jnp.dot(a, b, preferred_element_type=F32)


def norm_rows(values, gain):
    floats = values.astype(F32)
    scale = lax.rsqrt(jnp.mean(floats * floats, axis=-1, keepdims=True) + EPS)
    return (floats * scale * gain.astype(F32)).astype(BF16)


def kernel(
    n,
    cap,
    mix_hbm,
    mix_gain,
    pool_in_hbm,
    pool_map,
    pool_scale,
    pool_out_hbm,
    exp_hbm,
    exp_gain,
    group_router,
    expert_router,
    routes,
    gate_hbm,
    up_hbm,
    down_hbm,
    mix_out,
    exp_out,
    mix_in,
    pool_in,
    pool_out,
    pin,
    border,
    mixed,
    mpart,
    mrecv1,
    msend2,
    mrecv2,
    xin,
    normed,
    perm,
    pick,
    ysend,
    ybuf,
    zsend,
    rows,
    gate,
    up,
    down,
    gsum,
    usum,
    hidden,
    psend,
    precv,
    pown,
    zsend2,
    zbuf2,
    ysend2,
    ybuf2,
    local_sem,
    ys,
    yr,
    zs,
    zr,
    ys2,
    yr2,
    zs2,
    zr2,
    rs,
    rr,
    ps,
    pr,
    ws,
    wr,
    ms,
    mr,
):
    ep, tp = lax.axis_index("ep"), lax.axis_index("tp")
    z, yc = ep // n, ep % n
    devices = n * n
    mate = tp + 1 - 2 * (tp % 2)
    across = 3 - tp
    ahead, behind = (ep + 1) % devices, (ep + devices - 1) % devices
    tokens, model = xin.shape
    experts = expert_router.shape[1]
    slots = ysend.shape[0]
    block = slots // n
    width = model // CHUNKS
    hid = gate.shape[2]

    def cols(k):
        return pl.ds(pl.multiple_of(k * width, width), width)

    def part(index):
        return pl.ds(pl.multiple_of(index * block, 16), block)

    def remote(src, dst, send, recv, ep_to, tp_to):
        return pltpu.make_async_remote_copy(
            src_ref=src,
            dst_ref=dst,
            send_sem=send,
            recv_sem=recv,
            device_id={"ep": ep_to, "tp": tp_to},
            device_id_type=MESH,
        )

    local = [
        pltpu.make_async_copy(
            exp_hbm.at[pl.ds(pl.multiple_of(tp * tokens, 16), tokens)], xin, local_sem.at[0]
        ),
        pltpu.make_async_copy(mix_hbm, mix_in, local_sem.at[1]),
        pltpu.make_async_copy(pool_in_hbm, pool_in, local_sem.at[2]),
        pltpu.make_async_copy(pool_out_hbm, pool_out, local_sem.at[3]),
        pltpu.make_async_copy(gate_hbm.at[0], gate.at[0], local_sem.at[4]),
        pltpu.make_async_copy(up_hbm.at[0], up.at[0], local_sem.at[5]),
        pltpu.make_async_copy(down_hbm.at[0], down.at[0], local_sem.at[6]),
    ]
    for copy in local:
        copy.start()

    barrier = pltpu.get_barrier_semaphore()

    def greet(ep_to, tp_to):
        pl.semaphore_signal(
            barrier, inc=1, device_id={"ep": ep_to, "tp": tp_to}, device_id_type=MESH
        )

    @pl.loop(1, n)
    def _(d):
        greet(((z + d) % n) * n + yc, tp)
        greet(z * n + (yc + d) % n, tp)

    greet(ep, mate)
    greet(ep, across)
    greet(ahead, tp)
    greet(behind, tp)
    pl.semaphore_wait(barrier, 2 * (n - 1) + 4)

    def gate_copy(k):
        return remote(
            gate_hbm.at[0, cols(k)], gate.at[1, cols(k)], ws.at[0, k], wr.at[0, k], ep, mate
        )

    def up_copy(k):
        return remote(up_hbm.at[0, cols(k)], up.at[1, cols(k)], ws.at[1, k], wr.at[1, k], ep, mate)

    def down_copy(k):
        return remote(
            down_hbm.at[0, :, cols(k)],
            down.at[1, :, cols(k)],
            ws.at[2, k],
            wr.at[2, k],
            ep,
            mate,
        )

    @pl.loop(0, CHUNKS)
    def _(k):
        gate_copy(k).start()
        up_copy(k).start()

    @pl.loop(0, CHUNKS)
    def _(k):
        down_copy(k).start()

    def y_copy(src, dst, send, recv, k, d):
        to = (yc + d) % n
        return remote(
            src.at[part(to), cols(k)],
            dst.at[part(yc), cols(k)],
            send.at[k, d],
            recv.at[k, d],
            z * n + to,
            tp,
        )

    def z_copy(src, dst, send, recv, k, d):
        to = (z + d) % n
        return remote(
            src.at[part(to), cols(k)],
            dst.at[part(z), cols(k)],
            send.at[k, d],
            recv.at[k, d],
            to * n + yc,
            tp,
        )

    def start_all(copy, *args):
        @pl.loop(1, n)
        def _(d):
            copy(*args, d).start()

    def recv_all(copy, *args):
        @pl.loop(1, n)
        def _(d):
            copy(*args, d).wait_recv()

    def sent_all(copy, *args):
        @pl.loop(1, n)
        def _(d):
            copy(*args, d).wait_send()

    y_out = (y_copy, ysend, ybuf, ys, yr)
    z_out = (z_copy, zsend, rows.at[0], zs, zr)
    z_back = (z_copy, zsend2, zbuf2, zs2, zr2)
    y_back = (y_copy, ysend2, ybuf2, ys2, yr2)

    local[0].wait()
    normed[...] = norm_rows(xin[...], exp_gain[...])
    named = routes[pl.ds(pl.multiple_of(tp * tokens, 16), tokens), :]
    first, second = named[:, 0:1], named[:, 1:2]
    lanes = iota((tokens, experts), 1)
    routed = jnp.where((first == lanes) | (second == lanes), 1.0, 0.0)
    earlier = ones_where(iota((tokens, tokens), 1) < iota((tokens, tokens), 0))
    rank = dot(earlier, routed.astype(BF16))

    def slot_of(shape, dim):
        c = iota(shape, dim)
        y = over(c, n * cap)
        inner = c - y * (n * cap)
        zz = over(inner, cap)
        return zz * n + y, inner - zz * cap

    expert_c, place_c = slot_of((experts, slots), 1)
    spread = ones_where(iota((experts, slots), 0) == expert_c)
    ranks = dot((routed * (rank + 1.0)).astype(BF16), spread)
    expert_t, place_t = slot_of((tokens, slots), 1)
    chosen = jnp.where(ranks == (place_t + 1).astype(F32), 1.0, 0.0)
    pick[pl.ds(0, tokens), :] = jnp.where(first == expert_t, chosen, 0.0).astype(BF16)
    pick[pl.ds(tokens, tokens), :] = jnp.where(second == expert_t, chosen, 0.0).astype(BF16)
    chosen = chosen.astype(BF16)

    for k in range(CHUNKS):
        ysend[:, cols(k)] = lax.dot_general(
            chosen, normed[:, cols(k)], (((0,), (0,)), ((), ())), preferred_element_type=F32
        ).astype(BF16)
        start_all(*y_out, k)
        ybuf[part(yc), cols(k)] = ysend[part(yc), cols(k)]

    o = iota((slots, slots), 0)
    oa = over(o, block)
    ob = over(o - oa * block, cap)
    perm[...] = ones_where(iota((slots, slots), 1) == ob * block + oa * cap + (o - oa * block - ob * cap))

    def to_z(k):
        recv_all(*y_out, k)
        zsend[:, cols(k)] = dot(perm[...], ybuf[:, cols(k)]).astype(BF16)
        start_all(*z_out, k)
        rows[0, part(z), cols(k)] = zsend[part(z), cols(k)]

    local[1].wait()
    local[2].wait()
    total = mix_in.shape[0]
    step = 128

    @pl.loop(0, total // step)
    def _(b):
        at = pl.multiple_of(b * step, step)
        good = norm_rows(mix_in[pl.ds(at, step), :], mix_gain[...])
        pin[pl.ds(at + step, step), :] = dot(good, pool_in[...]).astype(BF16)

    border_copy = remote(
        pin.at[pl.ds(total + step - RIM, RIM)], border, ms.at[0], mr.at[0], ahead, tp
    )
    border_copy.start()

    to_z(0)

    border_copy.wait_recv()
    pin[pl.ds(0, step - RIM), :] = jnp.zeros((step - RIM, pin.shape[1]), BF16)
    edge = border[...].astype(F32)
    pin[pl.ds(step - RIM, RIM), :] = jnp.where(ep == 0, jnp.zeros_like(edge), edge).astype(BF16)
    window = jnp.left_shift(jnp.int32(2), tp)
    back = iota((step, 2 * step), 0) + step - iota((step, 2 * step), 1)
    band = ones_where((back >= 0) & (back < window))
    local[3].wait()

    @pl.loop(0, total // step)
    def _(b):
        at = pl.multiple_of(b * step, step)
        window_sum = dot(band, pin[pl.ds(at, 2 * step), :])
        position = ep * total + at + iota((step, 1), 0)
        count = jnp.minimum(position + 1, window).astype(F32)
        own = pin[pl.ds(at + step, step), :].astype(F32)
        pooled = (window_sum / count - own).astype(BF16)
        mixed[pl.ds(at, step), :] = (
            dot(pooled, pool_map[0]) * pool_scale[...].astype(F32)
        ).astype(BF16)

    to_z(1)

    half = total // 2
    quarter = total // 4
    away = pl.multiple_of((1 - tp // 2) * half, half)
    kept = pl.multiple_of((tp // 2) * half, half)

    def mix_project(start):
        @pl.loop(0, 2)
        def _(b):
            at = pl.multiple_of(start + b * quarter, quarter)
            mpart[pl.ds(at, quarter), :] = dot(mixed[pl.ds(at, quarter), :], pool_out[...]).astype(BF16)

    mix_project(away)
    mix_copy1 = remote(mpart.at[pl.ds(away, half)], mrecv1, ms.at[1], mr.at[1], ep, across)
    mix_copy1.start()
    to_z(2)
    mix_project(kept)
    to_z(3)

    gsum[...] = jnp.zeros_like(gsum)
    usum[...] = jnp.zeros_like(usum)
    for copy in local[4:]:
        copy.wait()

    def row_copy(k):
        return remote(rows.at[0, :, cols(k)], rows.at[1, :, cols(k)], rs.at[k], rr.at[k], ep, across)

    def accumulate(r, w, k):
        x = rows[r, :, cols(k)]
        gsum[r, w] += dot(x, gate[w, cols(k), :])
        usum[r, w] += dot(x, up[w, cols(k), :])

    @pl.loop(0, CHUNKS)
    def _(k):
        recv_all(*z_out, k)
        row_copy(k).start()
        accumulate(0, 0, k)

    mix_copy1.wait_recv()
    theirs = pl.multiple_of((mate % 2) * quarter, quarter)
    mine = pl.multiple_of((tp % 2) * quarter, quarter)
    msend2[...] = (
        mpart[pl.ds(kept + theirs, quarter), :].astype(F32)
        + mrecv1[pl.ds(theirs, quarter), :].astype(F32)
    ).astype(BF16)
    mix_copy2 = remote(msend2, mrecv2, ms.at[2], mr.at[2], ep, mate)
    mix_copy2.start()

    @pl.loop(0, CHUNKS)
    def _(k):
        gate_copy(k).wait_recv()
        up_copy(k).wait_recv()
        accumulate(0, 1, k)

    @pl.loop(0, CHUNKS)
    def _(k):
        row_copy(k).wait_recv()
        accumulate(1, 0, k)
        accumulate(1, 1, k)

    @pl.loop(0, 2)
    def _(r):
        @pl.loop(0, 2)
        def _(w):
            g = gsum[r, w]
            hidden[r, w] = (jax.nn.silu(g) * usum[r, w]).astype(BF16)

    def partial_copy(k):
        return remote(psend.at[:, cols(k)], precv.at[:, cols(k)], ps.at[k], pr.at[k], ep, across)

    def project(r, k):
        return dot(hidden[r, 0], down[0, :, cols(k)]) + dot(hidden[r, 1], down[1, :, cols(k)])

    def down_stage(k):
        down_copy(k).wait_recv()
        psend[:, cols(k)] = project(1, k).astype(BF16)
        partial_copy(k).start()
        pown[:, cols(k)] = project(0, k)

    def z_stage(k):
        partial_copy(k).wait_recv()
        zsend2[:, cols(k)] = (pown[:, cols(k)] + precv[:, cols(k)].astype(F32)).astype(BF16)
        start_all(*z_back, k)
        zbuf2[part(z), cols(k)] = zsend2[part(z), cols(k)]

    def y_stage(k):
        recv_all(*z_back, k)
        ysend2[:, cols(k)] = dot(perm[...], zbuf2[:, cols(k)]).astype(BF16)
        start_all(*y_back, k)
        ybuf2[part(yc), cols(k)] = ysend2[part(yc), cols(k)]

    own_rows = normed[...]
    group_exp = jnp.exp(dot(own_rows, group_router[...]))
    group_prob = group_exp / jnp.sum(group_exp, axis=1, keepdims=True)
    expert_exp = jnp.exp(dot(own_rows, expert_router[...]))
    groups = group_exp.shape[1]
    ratio = jnp.zeros_like(expert_exp)
    for q in range(groups):
        inside = over(lanes, experts // groups) == q
        within = jnp.sum(jnp.where(inside, expert_exp, 0.0), axis=1, keepdims=True)
        ratio = ratio + jnp.where(inside, group_prob[:, q : q + 1] / within, 0.0)
    prob = expert_exp * ratio
    picked0 = jnp.sum(jnp.where(first == lanes, prob, 0.0), axis=1, keepdims=True)
    picked1 = jnp.sum(jnp.where(second == lanes, prob, 0.0), axis=1, keepdims=True)
    weight0 = picked0 / (picked0 + picked1)
    weight1 = picked1 / (picked0 + picked1)

    def finish(k):
        recv_all(*y_back, k)
        both = dot(pick[...], ybuf2[:, cols(k)])
        exp_out[:, cols(k)] = (weight0 * both[:tokens] + weight1 * both[tokens:]).astype(BF16)

    stages = (down_stage, z_stage, y_stage, finish)
    for turn in range(CHUNKS + len(stages) - 1):
        for s, stage in enumerate(stages):
            if 0 <= turn - s < CHUNKS:
                stage(turn - s)

    mix_copy2.wait_recv()
    mix_out[...] = (
        mpart[pl.ds(kept + mine, quarter), :].astype(F32)
        + mrecv1[pl.ds(mine, quarter), :].astype(F32)
        + mrecv2[...].astype(F32)
    ).astype(BF16)

    border_copy.wait_send()
    mix_copy1.wait_send()
    mix_copy2.wait_send()

    @pl.loop(0, CHUNKS)
    def _(k):
        gate_copy(k).wait_send()
        up_copy(k).wait_send()
        down_copy(k).wait_send()
        row_copy(k).wait_send()
        partial_copy(k).wait_send()
        sent_all(*y_out, k)
        sent_all(*z_out, k)
        sent_all(*z_back, k)
        sent_all(*y_back, k)


def on_device(n, *args):
    (
        mixer_input,
        mixer_gain,
        pool_in,
        pool_map,
        pool_scale,
        pool_out,
        expert_input,
        expert_gain,
        group_router,
        expert_router,
        routes,
        gate_weight,
        up_weight,
        down_weight,
    ) = args
    total, model = mixer_input.shape
    channels = pool_in.shape[1]
    tokens = expert_input.shape[0] // 4
    experts = expert_router.shape[1]
    cap = 4 * tokens // experts
    slots = cap * experts
    hid = gate_weight.shape[2]
    vmem = pl.BlockSpec(memory_space=pltpu.VMEM)
    hbm = pl.BlockSpec(memory_space=pl.ANY)
    dma = pltpu.SemaphoreType.DMA
    each = dma((CHUNKS, n))
    return pl.pallas_call(
        functools.partial(kernel, n, cap),
        out_shape=(
            jax.ShapeDtypeStruct((total // 4, model), BF16),
            jax.ShapeDtypeStruct((tokens, model), BF16),
        ),
        in_specs=[hbm, vmem, hbm, vmem, vmem, hbm, hbm, vmem, vmem, vmem, vmem, hbm, hbm, hbm],
        out_specs=(vmem, vmem),
        scratch_shapes=[
            pltpu.VMEM((total, model), BF16),
            pltpu.VMEM((model, channels), BF16),
            pltpu.VMEM((channels, model), BF16),
            pltpu.VMEM((total + 128, channels), BF16),
            pltpu.VMEM((RIM, channels), BF16),
            pltpu.VMEM((total, channels), BF16),
            pltpu.VMEM((total, model), BF16),
            pltpu.VMEM((total // 2, model), BF16),
            pltpu.VMEM((total // 4, model), BF16),
            pltpu.VMEM((total // 4, model), BF16),
            pltpu.VMEM((tokens, model), BF16),
            pltpu.VMEM((tokens, model), BF16),
            pltpu.VMEM((slots, slots), BF16),
            pltpu.VMEM((2 * tokens, slots), BF16),
            pltpu.VMEM((slots, model), BF16),
            pltpu.VMEM((slots, model), BF16),
            pltpu.VMEM((slots, model), BF16),
            pltpu.VMEM((2, slots, model), BF16),
            pltpu.VMEM((2, model, hid), BF16),
            pltpu.VMEM((2, model, hid), BF16),
            pltpu.VMEM((2, hid, model), BF16),
            pltpu.VMEM((2, 2, slots, hid), F32),
            pltpu.VMEM((2, 2, slots, hid), F32),
            pltpu.VMEM((2, 2, slots, hid), BF16),
            pltpu.VMEM((slots, model), BF16),
            pltpu.VMEM((slots, model), BF16),
            pltpu.VMEM((slots, model), F32),
            pltpu.VMEM((slots, model), BF16),
            pltpu.VMEM((slots, model), BF16),
            pltpu.VMEM((slots, model), BF16),
            pltpu.VMEM((slots, model), BF16),
            dma((7,)),
            each,
            each,
            each,
            each,
            each,
            each,
            each,
            each,
            dma((CHUNKS,)),
            dma((CHUNKS,)),
            dma((CHUNKS,)),
            dma((CHUNKS,)),
            dma((3, CHUNKS)),
            dma((3, CHUNKS)),
            dma((3,)),
            dma((3,)),
        ],
        compiler_params=pltpu.CompilerParams(
            collective_id=0, has_side_effects=True, vmem_limit_bytes=60 * 1024 * 1024
        ),
    )(
        mixer_input,
        mixer_gain.reshape(1, model),
        pool_in,
        pool_map,
        pool_scale.reshape(1, channels),
        pool_out,
        expert_input,
        expert_gain.reshape(1, model),
        group_router,
        expert_router,
        routes,
        gate_weight,
        up_weight,
        down_weight,
    )


def solution(mesh):
    n = 1
    while n * n < mesh.shape["ep"]:
        n += 1
    return jax.shard_map(
        functools.partial(on_device, n),
        mesh=mesh,
        in_specs=(
            P("ep", None),
            P(),
            P(None, "tp"),
            P("tp", None, None),
            P("tp"),
            P("tp", None),
            P("ep", None),
            P(),
            P(),
            P(),
            P("ep", None),
            P("ep", None, "tp"),
            P("ep", None, "tp"),
            P("ep", "tp", None),
        ),
        out_specs=(P(("ep", "tp"), None), P(("ep", "tp"), None)),
        check_vma=False,
    )
```

```python
import functools

import jax
import jax.numpy as jnp
from jax import lax
from jax.experimental import pallas as pl
from jax.experimental.pallas import tpu as pltpu
from jax.sharding import PartitionSpec as P

EPS = 1e-06
RIM = 16
CHUNKS = 8
Z_FIRST = 2
PIECES = 4
ACROSS_FIRST = 1
BACK = (256,) * 7 + (128, 128)
scope = jax.named_scope
MESH = pl.DeviceIdType.MESH
F32 = jnp.float32
BF16 = jnp.bfloat16


def iota(shape, dim):
    return lax.broadcasted_iota(jnp.int32, shape, dim)


def over(value, divisor):
    return (value * (-(-65536 // divisor))) >> 16


def ones_where(mask):
    return jnp.where(mask, 1.0, 0.0).astype(BF16)


def dot(a, b):
    return jnp.dot(a, b, preferred_element_type=F32)


def dot_t(a, b):
    return lax.dot_general(a, b, (((1,), (1,)), ((), ())), preferred_element_type=F32)


def norm_rows(values, gain):
    floats = values.astype(F32)
    scale = lax.rsqrt(jnp.mean(floats * floats, axis=-1, keepdims=True) + EPS)
    return (floats * scale * gain.astype(F32)[None, :]).astype(BF16)


def kernel(
    n,
    cap,
    mix_hbm,
    mix_gain,
    pool_in_hbm,
    pool_map,
    pool_scale,
    pool_out_hbm,
    exp_hbm,
    exp_gain,
    group_router,
    expert_router,
    routes,
    gate_hbm,
    up_hbm,
    down_hbm,
    mix_out,
    exp_out,
    mix_in,
    pool_in,
    pool_out,
    pin,
    border,
    mixed,
    mpart,
    mrecv1,
    msend2,
    mrecv2,
    xin,
    normed,
    perm,
    pick,
    ysend,
    ybuf,
    zsend,
    rows,
    gate,
    up,
    down,
    gsum,
    usum,
    hidden,
    psend,
    precv,
    pown,
    zsend2,
    zbuf2,
    ysend2,
    ybuf2,
    local_sem,
    ys,
    yr,
    zs,
    zr,
    ys2,
    yr2,
    zs2,
    zr2,
    rs,
    rr,
    ps,
    pr,
    ws,
    wr,
    ms,
    mr,
    mix1s,
    mix1r,
    mix2s,
    mix2r,
    yland,
    exp_fin,
    mix_fin,
    exp_sem,
    mix_sem,
):
    ep, tp = lax.axis_index("ep"), lax.axis_index("tp")
    z, yc = ep // n, ep % n
    devices = n * n
    mate = tp + 1 - 2 * (tp % 2)
    across = 3 - tp
    ahead, behind = (ep + 1) % devices, (ep + devices - 1) % devices
    tokens, model = xin.shape
    experts = expert_router.shape[0]
    slots = ysend.shape[0]
    block = slots // n
    width = model // CHUNKS
    hid = gate.shape[2]

    def cols(k):
        return pl.ds(pl.multiple_of(k * width, width), width)

    def part(index):
        return pl.ds(pl.multiple_of(index * block, 16), block)

    def remote(src, dst, send, recv, ep_to, tp_to):
        return pltpu.make_async_remote_copy(
            src_ref=src,
            dst_ref=dst,
            send_sem=send,
            recv_sem=recv,
            device_id={"ep": ep_to, "tp": tp_to},
            device_id_type=MESH,
        )

    local = [
        pltpu.make_async_copy(
            exp_hbm.at[pl.ds(pl.multiple_of(tp * tokens, 16), tokens)], xin, local_sem.at[0]
        ),
        pltpu.make_async_copy(mix_hbm, mix_in, local_sem.at[1]),
        pltpu.make_async_copy(pool_in_hbm, pool_in, local_sem.at[2]),
        pltpu.make_async_copy(pool_out_hbm, pool_out, local_sem.at[3]),
        pltpu.make_async_copy(gate_hbm.at[0], gate.at[0], local_sem.at[4]),
        pltpu.make_async_copy(up_hbm.at[0], up.at[0], local_sem.at[5]),
        pltpu.make_async_copy(down_hbm.at[0], down.at[0], local_sem.at[6]),
    ]
    for copy in local:
        copy.start()

    barrier = pltpu.get_barrier_semaphore()

    def greet(ep_to, tp_to):
        pl.semaphore_signal(
            barrier, inc=1, device_id={"ep": ep_to, "tp": tp_to}, device_id_type=MESH
        )

    @pl.loop(1, n)
    def _(d):
        greet(((z + d) % n) * n + yc, tp)
        greet(z * n + (yc + d) % n, tp)

    greet(ep, mate)
    greet(ep, across)
    greet(ahead, tp)
    greet(behind, tp)
    def gate_copy(k):
        return remote(
            gate_hbm.at[0, cols(k)], gate.at[1, cols(k)], ws.at[0, k], wr.at[0, k], ep, mate
        )

    def up_copy(k):
        return remote(up_hbm.at[0, cols(k)], up.at[1, cols(k)], ws.at[1, k], wr.at[1, k], ep, mate)

    def down_copy(k):
        return remote(
            down_hbm.at[0, :, cols(k)],
            down.at[1, :, cols(k)],
            ws.at[2, k],
            wr.at[2, k],
            ep,
            mate,
        )

    def y_copy(src, dst, send, recv, k, at, d):
        to = (yc + d) % n
        return remote(src.at[part(to), at], dst.at[part(yc), at], send, recv.at[k], z * n + to, tp)

    def z_copy(src, dst, send, recv, k, at, d):
        to = (z + d) % n
        return remote(src.at[part(to), at], dst.at[part(z), at], send, recv.at[k], to * n + yc, tp)

    def start_all(copy, *args):
        @pl.loop(1, n)
        def _(d):
            copy(*args, d).start()

    others = pl.ds(0, slots - block)

    def recv_all(copy, src, dst, send, recv, k, at):
        remote(src.at[others, at], dst.at[others, at], send, recv.at[k], ep, mate).wait_recv()

    def sent_all(src, send):
        remote(src.at[others], src.at[others], send, zr.at[0], ep, mate).wait_send()

    y_out = (y_copy, ysend, ybuf, ys, yr)
    z_out = (z_copy, zsend, rows.at[0], zs, zr)
    z_early = (z_copy, zsend, ybuf, zs, zr)
    y_late = (y_copy, ysend, yland, ys, yr)
    z_back = (z_copy, zsend2, zbuf2, zs2, zr2)
    y_back = (y_copy, ysend2, ybuf2, ys2, yr2)

    local[0].wait()
    normed[...] = norm_rows(xin[...], exp_gain[...])
    everyone = routes.shape[1]
    named = routes[...].astype(F32)
    here = iota((tokens, everyone), 1) == tp * tokens + iota((tokens, everyone), 0)
    first, second = [
        jnp.sum(jnp.where(here, named[j : j + 1, :], 0.0), axis=1, keepdims=True).astype(jnp.int32)
        for j in range(2)
    ]
    here = iota((everyone, tokens), 0) == tp * tokens + iota((everyone, tokens), 1)
    named = dot(named.astype(BF16), ones_where(here)).astype(jnp.int32)
    lanes = iota((experts, tokens), 0)
    routed = jnp.where((named[0:1, :] == lanes) | (named[1:2, :] == lanes), 1.0, 0.0)
    earlier = ones_where(iota((tokens, tokens), 0) < iota((tokens, tokens), 1))
    rank = (routed * (dot(routed.astype(BF16), earlier) + 1.0)).astype(BF16)

    def slot_of(shape, dim):
        c = iota(shape, dim)
        outer = over(c, n * cap)
        inner = over(c - outer * (n * cap), cap)
        return outer, inner, c - outer * (n * cap) - inner * cap

    def packing(z_major):
        outer, inner, _ = slot_of((slots, experts), 0)
        expert = outer * n + inner if z_major else inner * n + outer
        ranks = dot(ones_where(iota((slots, experts), 1) == expert), rank)
        return ones_where(ranks == (slot_of((slots, tokens), 0)[2] + 1).astype(F32))

    early = pl.ds(0, Z_FIRST * width)
    late = pl.ds(Z_FIRST * width, model - Z_FIRST * width)
    zsend[:, early] = dot(packing(True), normed[:, early]).astype(BF16)
    ysend[:, late] = dot(packing(False), normed[:, late]).astype(BF16)

    local[1].wait()
    local[2].wait()
    total = mix_in.shape[0]
    step = 128

    @pl.loop(0, total // step)
    def _(b):
        at = pl.multiple_of(b * step, step)
        good = norm_rows(mix_in[pl.ds(at, step), :], mix_gain[...])
        pin[pl.ds(at + step, step), :] = dot(good, pool_in[...]).astype(BF16)

    border_copy = remote(
        pin.at[pl.ds(total + step - RIM, RIM)], border, ms.at[0], mr.at[0], ahead, tp
    )

    with scope("barrier"):
        pl.semaphore_wait(barrier, 2 * (n - 1) + 4)
    border_copy.start()

    for k in range(Z_FIRST):
        start_all(*z_early, k, cols(k))
    for k in range(Z_FIRST, Z_FIRST + 3):
        start_all(*y_out, k, cols(k))

    @pl.loop(0, CHUNKS)
    def _(k):
        gate_copy(k).start()
        up_copy(k).start()

    @pl.loop(0, CHUNKS)
    def _(k):
        down_copy(k).start()

    ybuf[part(z), early] = zsend[part(z), early]
    ybuf[part(yc), late] = ysend[part(yc), late]

    outer, inner, place = slot_of((slots, slots), 0)
    perm[...] = ones_where(iota((slots, slots), 1) == inner * block + outer * cap + place)

    def to_y(k):
        with scope("wait_z"):
            recv_all(*z_early, k, cols(k))
        ysend[:, cols(k)] = dot(perm[...], ybuf[:, cols(k)]).astype(BF16)
        start_all(*y_late, k, cols(k))
        yland[part(yc), cols(k)] = ysend[part(yc), cols(k)]

    def to_z(k):
        with scope("wait_y"):
            recv_all(*y_out, k, cols(k))
        zsend[:, cols(k)] = dot(perm[...], ybuf[:, cols(k)]).astype(BF16)
        start_all(*z_out, k, cols(k))
        rows[0, part(z), cols(k)] = zsend[part(z), cols(k)]
        part_copy(k, 0).start()

    def part_copy(k, d):
        at = part((z + d) % n)
        return remote(
            rows.at[0, at, cols(k)], rows.at[1, at, cols(k)], rs.at[k], rr.at[k], ep, across
        )

    def row_copy(k):
        return remote(rows.at[0, :, cols(k)], rows.at[1, :, cols(k)], rs.at[k], rr.at[k], ep, across)

    def arrive_late(k):
        with scope("wait_y"):
            recv_all(*y_late, k, cols(k))
        rows[0, :, cols(k)] = dot(perm[...], yland[:, cols(k)]).astype(BF16)
        row_copy(k).start()

    def arrive(k):
        with scope("wait_z"):
            recv_all(*z_out, k, cols(k))

        @pl.loop(1, n)
        def _(d):
            part_copy(k, d).start()


    with scope("wait_border"):
        border_copy.wait_recv()
    pin[pl.ds(0, step - RIM), :] = jnp.zeros((step - RIM, pin.shape[1]), BF16)
    edge = border[...].astype(F32)
    pin[pl.ds(step - RIM, RIM), :] = jnp.where(ep == 0, jnp.zeros_like(edge), edge).astype(BF16)
    window = jnp.left_shift(jnp.int32(2), tp)
    back = iota((step, 2 * step), 0) + step - iota((step, 2 * step), 1)
    band = ones_where((back >= 0) & (back < window))
    local[3].wait()

    @pl.loop(0, total // step)
    def _(b):
        at = pl.multiple_of(b * step, step)
        window_sum = dot(band, pin[pl.ds(at, 2 * step), :])
        position = ep * total + at + iota((step, 1), 0)
        count = jnp.minimum(position + 1, window).astype(F32)
        own = pin[pl.ds(at + step, step), :].astype(F32)
        pooled = (window_sum / count - own).astype(BF16)
        mixed[pl.ds(at, step), :] = (
            dot(pooled, pool_map[0]) * pool_scale[...].astype(F32)[None, :]
        ).astype(BF16)

    quarter = total // 4
    wide = model // PIECES

    def quarter_rows(index):
        return pl.ds(pl.multiple_of(index * quarter, quarter), quarter)

    def piece(j):
        return pl.ds(j * wide, wide)

    def steps(j):
        return (across, mate) if j < ACROSS_FIRST else (mate, across)

    def mix_copy1(j, s):
        return remote(
            mpart.at[quarter_rows(3 - mate if s else steps(j)[0]), piece(j)],
            mrecv1.at[s, :, piece(j)],
            mix1s.at[j, s],
            mix1r.at[j, s],
            ep,
            steps(j)[0],
        )

    def mix_copy2(j):
        return remote(
            msend2.at[:, piece(j)], mrecv2.at[:, piece(j)], mix2s.at[j], mix2r.at[j], ep, steps(j)[1]
        )

    def mix_project(j):
        mpart[:, piece(j)] = dot(mixed[...], pool_out[:, piece(j)]).astype(BF16)
        mix_copy1(j, 0).start()
        mix_copy1(j, 1).start()

    def mix_stage(j):
        with scope("wait_mix1"):
            mix_copy1(j, 0).wait_recv()
            mix_copy1(j, 1).wait_recv()
        msend2[:, piece(j)] = (
            mpart[quarter_rows(steps(j)[1]), piece(j)].astype(F32)
            + mrecv1[1, :, piece(j)].astype(F32)
        ).astype(BF16)
        mix_copy2(j).start()

    def mix_out_copy(j):
        return pltpu.make_async_copy(
            mix_fin.at[:, piece(j)], mix_out.at[:, piece(j)], mix_sem.at[j]
        )

    def mix_finish(j):
        with scope("wait_mix2"):
            mix_copy2(j).wait_recv()
        mix_fin[:, piece(j)] = (
            mpart[quarter_rows(tp), piece(j)].astype(F32)
            + mrecv1[0, :, piece(j)].astype(F32)
            + mrecv2[:, piece(j)].astype(F32)
        ).astype(BF16)
        mix_out_copy(j).start()

    for j in range(ACROSS_FIRST):
        mix_project(j)
    to_z(Z_FIRST)
    to_z(Z_FIRST + 1)
    to_y(0)
    start_all(*y_out, Z_FIRST + 3, cols(Z_FIRST + 3))
    to_z(Z_FIRST + 2)
    for j in range(ACROSS_FIRST, PIECES):
        mix_project(j)
    to_y(1)
    for k in range(Z_FIRST + 4, CHUNKS):
        start_all(*y_out, k, cols(k))
    arrive_late(0)
    to_z(Z_FIRST + 3)
    arrive_late(1)
    to_z(Z_FIRST + 4)
    arrive(Z_FIRST)
    to_z(Z_FIRST + 5)

    gsum[...] = jnp.zeros_like(gsum)
    usum[...] = jnp.zeros_like(usum)
    for copy in local[4:]:
        copy.wait()

    def accumulate(r, w, k):
        x = rows[r, :, cols(k)]
        gsum[r, w] += dot(x, gate[w, cols(k), :])
        usum[r, w] += dot(x, up[w, cols(k), :])

    @pl.loop(0, Z_FIRST + 1)
    def _(k):
        accumulate(0, 0, k)

    @pl.loop(Z_FIRST + 1, CHUNKS)
    def _(k):
        arrive(k)
        accumulate(0, 0, k)

    for j in range(ACROSS_FIRST):
        mix_stage(j)

    lanes = iota((tokens, experts), 1)
    routed = jnp.where((first == lanes) | (second == lanes), 1.0, 0.0)
    earlier = ones_where(iota((tokens, tokens), 1) < iota((tokens, tokens), 0))
    rank = (routed * (dot(earlier, routed.astype(BF16)) + 1.0)).astype(BF16)
    outer, inner, _ = slot_of((experts, slots), 1)
    ranks = dot(rank, ones_where(iota((experts, slots), 0) == inner * n + outer))
    outer, inner, place = slot_of((tokens, slots), 1)
    expert = inner * n + outer
    chosen = ranks == (place + 1).astype(F32)
    pick[pl.ds(0, tokens), :] = ones_where(chosen & (first == expert))
    pick[pl.ds(tokens, tokens), :] = ones_where(chosen & (second == expert))
    own_rows = normed[...]
    group_exp = jnp.exp(dot_t(own_rows, group_router[...]))
    group_prob = group_exp / jnp.sum(group_exp, axis=1, keepdims=True)
    expert_exp = jnp.exp(dot_t(own_rows, expert_router[...]))
    groups = group_exp.shape[1]
    ratio = jnp.zeros_like(expert_exp)
    for q in range(groups):
        inside = over(lanes, experts // groups) == q
        within = jnp.sum(jnp.where(inside, expert_exp, 0.0), axis=1, keepdims=True)
        ratio = ratio + jnp.where(inside, group_prob[:, q : q + 1] / within, 0.0)
    prob = expert_exp * ratio
    picked0 = jnp.sum(jnp.where(first == lanes, prob, 0.0), axis=1, keepdims=True)
    picked1 = jnp.sum(jnp.where(second == lanes, prob, 0.0), axis=1, keepdims=True)
    weight0 = picked0 / (picked0 + picked1)
    weight1 = picked1 / (picked0 + picked1)

    @pl.loop(0, CHUNKS)
    def _(k):
        with scope("wait_w"):
            gate_copy(k).wait_recv()
            up_copy(k).wait_recv()
        accumulate(0, 1, k)
        with scope("wait_r"):
            row_copy(k).wait_recv()
        accumulate(1, 0, k)
        accumulate(1, 1, k)

    @pl.loop(0, 2)
    def _(r):
        @pl.loop(0, 2)
        def _(w):
            g = gsum[r, w]
            hidden[r, w] = (jax.nn.silu(g) * usum[r, w]).astype(BF16)

    spans = [pl.ds(sum(BACK[:k]), BACK[k]) for k in range(len(BACK))]

    def partial_copy(k):
        at = spans[k]
        return remote(psend.at[:, at], precv.at[:, at], ps.at[k], pr.at[k], ep, across)

    def project(r, at):
        return dot(hidden[r, 0], down[0, :, at]) + dot(hidden[r, 1], down[1, :, at])

    def down_stage(k):
        at = spans[k]
        if at.start % width == 0:
            with scope("wait_down"):
                down_copy(at.start // width).wait_recv()
        psend[:, at] = project(1, at).astype(BF16)
        partial_copy(k).start()
        pown[:, at] = project(0, at)

    def z_stage(k):
        at = spans[k]
        with scope("wait_part"):
            partial_copy(k).wait_recv()
        zsend2[:, at] = (pown[:, at] + precv[:, at].astype(F32)).astype(BF16)
        start_all(*z_back, k, at)
        zbuf2[part(z), at] = zsend2[part(z), at]

    def y_stage(k):
        at = spans[k]
        with scope("wait_zb"):
            recv_all(*z_back, k, at)
        ysend2[:, at] = dot(perm[...], zbuf2[:, at]).astype(BF16)
        start_all(*y_back, k, at)
        ybuf2[part(yc), at] = ysend2[part(yc), at]

    def exp_copy(k):
        at = spans[k]
        return pltpu.make_async_copy(exp_fin.at[:, at], exp_out.at[:, at], exp_sem.at[k])

    def finish(k):
        at = spans[k]
        with scope("wait_yb"):
            recv_all(*y_back, k, at)
        both = dot(pick[...], ybuf2[:, at])
        exp_fin[:, at] = (weight0 * both[:tokens] + weight1 * both[tokens:]).astype(BF16)
        exp_copy(k).start()

    stages = ((down_stage, 0), (z_stage, 2), (y_stage, 4), (finish, 6))
    for turn in range(len(BACK) + 6):
        for stage, later in stages:
            if 0 <= turn - later < len(BACK):
                with scope(stage.__name__):
                    stage(turn - later)
        if 0 <= turn - len(BACK) + 1 < PIECES - ACROSS_FIRST:
            mix_stage(turn - len(BACK) + 1 + ACROSS_FIRST)
    for j in range(PIECES):
        mix_finish(j)

    with scope("sent"):
        border_copy.wait_send()
        for src, send in ((ysend, ys), (zsend, zs), (ysend2, ys2), (zsend2, zs2)):
            sent_all(src, send)

    for j in range(PIECES):
        mix_copy1(j, 0).wait_send()
        mix_copy1(j, 1).wait_send()
        mix_copy2(j).wait_send()

    @pl.loop(0, CHUNKS)
    def _(k):
        gate_copy(k).wait_send()
        up_copy(k).wait_send()
        down_copy(k).wait_send()
        row_copy(k).wait_send()

    for k in range(len(BACK)):
        partial_copy(k).wait_send()
        exp_copy(k).wait()

    for j in range(PIECES):
        mix_out_copy(j).wait()


def write_out(mix_from, exp_from, mix_to, exp_to, mix_held, exp_held, in_sem, out_sem):
    whole = ((mix_from, mix_held, mix_to), (exp_from, exp_held, exp_to))

    def copies(i, h):
        source, held, target = whole[i]
        size = held.shape[0] // 2
        at = pl.ds(h * size, size)
        return (
            pltpu.make_async_copy(source.at[at], held.at[at], in_sem.at[i, h]),
            pltpu.make_async_copy(held.at[at], target.at[at], out_sem.at[i, h]),
        )

    each = [copies(i, h) for i in range(2) for h in range(2)]
    for copy_in, _ in each:
        copy_in.start()
    for copy_in, copy_out in each:
        copy_in.wait()
        copy_out.start()
    for _, copy_out in each:
        copy_out.wait()


def on_device(n, *args):
    (
        mixer_input,
        mixer_gain,
        pool_in,
        pool_map,
        pool_scale,
        pool_out,
        expert_input,
        expert_gain,
        group_router,
        expert_router,
        routes,
        gate_weight,
        up_weight,
        down_weight,
    ) = args
    total, model = mixer_input.shape
    channels = pool_in.shape[1]
    tokens = expert_input.shape[0] // 4
    experts = expert_router.shape[1]
    cap = 4 * tokens // experts
    slots = cap * experts
    hid = gate_weight.shape[2]
    vmem = pl.BlockSpec(memory_space=pltpu.VMEM)
    hbm = pl.BlockSpec(memory_space=pl.ANY)
    dma = pltpu.SemaphoreType.DMA
    each, back = dma((CHUNKS,)), dma((len(BACK),))
    sent = pl.pallas_call(
        functools.partial(kernel, n, cap),
        out_shape=(
            jax.ShapeDtypeStruct((total // 4, model), BF16),
            jax.ShapeDtypeStruct((tokens, model), BF16),
        ),
        in_specs=[hbm, vmem, hbm, vmem, vmem, hbm, hbm, vmem, vmem, vmem, vmem, hbm, hbm, hbm],
        out_specs=(hbm, hbm),
        scratch_shapes=[
            pltpu.VMEM((total, model), BF16),
            pltpu.VMEM((model, channels), BF16),
            pltpu.VMEM((channels, model), BF16),
            pltpu.VMEM((total + 128, channels), BF16),
            pltpu.VMEM((RIM, channels), BF16),
            pltpu.VMEM((total, channels), BF16),
            pltpu.VMEM((total, model), BF16),
            pltpu.VMEM((2, total // 4, model), BF16),
            pltpu.VMEM((total // 4, model), BF16),
            pltpu.VMEM((total // 4, model), BF16),
            pltpu.VMEM((tokens, model), BF16),
            pltpu.VMEM((tokens, model), BF16),
            pltpu.VMEM((slots, slots), BF16),
            pltpu.VMEM((2 * tokens, slots), BF16),
            pltpu.VMEM((slots, model), BF16),
            pltpu.VMEM((slots, model), BF16),
            pltpu.VMEM((slots, model), BF16),
            pltpu.VMEM((2, slots, model), BF16),
            pltpu.VMEM((2, model, hid), BF16),
            pltpu.VMEM((2, model, hid), BF16),
            pltpu.VMEM((2, hid, model), BF16),
            pltpu.VMEM((2, 2, slots, hid), F32),
            pltpu.VMEM((2, 2, slots, hid), F32),
            pltpu.VMEM((2, 2, slots, hid), BF16),
            pltpu.VMEM((slots, model), BF16),
            pltpu.VMEM((slots, model), BF16),
            pltpu.VMEM((slots, model), F32),
            pltpu.VMEM((slots, model), BF16),
            pltpu.VMEM((slots, model), BF16),
            pltpu.VMEM((slots, model), BF16),
            pltpu.VMEM((slots, model), BF16),
            dma((7,)),
            dma,
            each,
            dma,
            each,
            dma,
            back,
            dma,
            back,
            each,
            each,
            back,
            back,
            dma((3, CHUNKS)),
            dma((3, CHUNKS)),
            dma((1,)),
            dma((1,)),
            dma((PIECES, 2)),
            dma((PIECES, 2)),
            dma((PIECES,)),
            dma((PIECES,)),
            pltpu.VMEM((slots, Z_FIRST * model // CHUNKS), BF16),
            pltpu.VMEM((tokens, model), BF16),
            pltpu.VMEM((total // 4, model), BF16),
            dma((len(BACK),)),
            dma((PIECES,)),
        ],
        compiler_params=pltpu.CompilerParams(
            collective_id=0, has_side_effects=True, vmem_limit_bytes=60 * 1024 * 1024
        ),
    )(
        mixer_input,
        mixer_gain,
        pool_in,
        pool_map,
        pool_scale,
        pool_out,
        expert_input,
        expert_gain,
        group_router.T,
        expert_router.T,
        routes.T,
        gate_weight,
        up_weight,
        down_weight,
    )
    shapes = [(total // 4, model), (tokens, model)]
    return pl.pallas_call(
        write_out,
        out_shape=tuple(jax.ShapeDtypeStruct(shape, BF16) for shape in shapes),
        in_specs=[hbm, hbm],
        out_specs=(hbm, hbm),
        scratch_shapes=[pltpu.VMEM(shape, BF16) for shape in shapes] + [dma((2, 2)), dma((2, 2))],
        cost_estimate=pl.CostEstimate(flops=0, bytes_accessed=4 * 224 * model, transcendentals=0),
    )(*sent)


def solution(mesh):
    n = 1
    while n * n < mesh.shape["ep"]:
        n += 1
    return jax.shard_map(
        functools.partial(on_device, n),
        mesh=mesh,
        in_specs=(
            P("ep", None),
            P(),
            P(None, "tp"),
            P("tp", None, None),
            P("tp"),
            P("tp", None),
            P("ep", None),
            P(),
            P(),
            P(),
            P("ep", None),
            P("ep", None, "tp"),
            P("ep", None, "tp"),
            P("ep", "tp", None),
        ),
        out_specs=(P(("ep", "tp"), None), P(("ep", "tp"), None)),
        check_vma=False,
    )
```

```python
import functools

import jax
import jax.numpy as jnp
from jax import lax
from jax.experimental import pallas as pl
from jax.experimental.pallas import tpu as pltpu
from jax.sharding import PartitionSpec as P

EPS = 1e-06
RIM = 16
CHUNKS = 8
Z_FIRST = 2
PIECES = 4
ACROSS_FIRST = 1
BACK = (128, 128) + (256,) * 6 + (128, 128)
scope = jax.named_scope
MESH = pl.DeviceIdType.MESH
F32 = jnp.float32
BF16 = jnp.bfloat16


def iota(shape, dim):
    return lax.broadcasted_iota(jnp.int32, shape, dim)


def over(value, divisor):
    return (value * (-(-65536 // divisor))) >> 16


def ones_where(mask):
    return jnp.where(mask, 1.0, 0.0).astype(BF16)


def dot(a, b):
    return jnp.dot(a, b, preferred_element_type=F32)


def dot_t(a, b):
    return lax.dot_general(a, b, (((1,), (1,)), ((), ())), preferred_element_type=F32)


def norm_rows(values, gain):
    floats = values.astype(F32)
    scale = lax.rsqrt(jnp.mean(floats * floats, axis=-1, keepdims=True) + EPS)
    return (floats * scale * gain.astype(F32)[None, :]).astype(BF16)


def kernel(
    n,
    cap,
    mix_hbm,
    mix_gain_hbm,
    pool_in_hbm,
    pool_map_hbm,
    pool_scale_hbm,
    pool_out_hbm,
    exp_hbm,
    exp_gain_hbm,
    group_router_hbm,
    expert_router_hbm,
    routes_hbm,
    gate_hbm,
    up_hbm,
    down_hbm,
    mix_out,
    exp_out,
    mix_in,
    pool_in,
    pool_out,
    pin,
    border,
    mixed,
    mpart,
    mrecv1,
    msend2,
    mrecv2,
    xin,
    normed,
    perm,
    pick,
    ysend,
    ybuf,
    zsend,
    rows,
    gate,
    up,
    down,
    gsum,
    usum,
    hidden,
    psend,
    precv,
    pown,
    zsend2,
    zbuf2,
    ysend2,
    ybuf2,
    local_sem,
    ys,
    yr,
    zs,
    zr,
    ys2,
    yr2,
    zs2,
    zr2,
    rs,
    rr,
    ps,
    pr,
    ws,
    wr,
    ms,
    mr,
    mix1s,
    mix1r,
    mix2s,
    mix2r,
    yland,
    exp_fin,
    mix_fin,
    exp_sem,
    mix_sem,
    ds,
    dr,
    mix_gain,
    pool_map,
    pool_scale,
    exp_gain,
    group_router,
    expert_router,
    routes,
):
    ep, tp = lax.axis_index("ep"), lax.axis_index("tp")
    z, yc = ep // n, ep % n
    devices = n * n
    mate = tp + 1 - 2 * (tp % 2)
    across = 3 - tp
    ahead, behind = (ep + 1) % devices, (ep + devices - 1) % devices
    tokens, model = xin.shape
    experts = expert_router.shape[0]
    slots = ysend.shape[0]
    block = slots // n
    width = model // CHUNKS
    hid = gate.shape[2]

    def cols(k):
        return pl.ds(pl.multiple_of(k * width, width), width)

    def part(index):
        return pl.ds(pl.multiple_of(index * block, 16), block)

    def remote(src, dst, send, recv, ep_to, tp_to):
        return pltpu.make_async_remote_copy(
            src_ref=src,
            dst_ref=dst,
            send_sem=send,
            recv_sem=recv,
            device_id={"ep": ep_to, "tp": tp_to},
            device_id_type=MESH,
        )

    barrier = pltpu.get_barrier_semaphore()

    def greet(ep_to, tp_to):
        pl.semaphore_signal(
            barrier, inc=1, device_id={"ep": ep_to, "tp": tp_to}, device_id_type=MESH
        )

    @pl.loop(1, n)
    def _(d):
        greet(((z + d) % n) * n + yc, tp)
        greet(z * n + (yc + d) % n, tp)

    greet(ep, mate)
    greet(ep, across)
    greet(ahead, tp)
    greet(behind, tp)
    local = [
        pltpu.make_async_copy(
            exp_hbm.at[pl.ds(pl.multiple_of(tp * tokens, 16), tokens)], xin, local_sem.at[0]
        ),
        pltpu.make_async_copy(mix_hbm, mix_in, local_sem.at[1]),
        pltpu.make_async_copy(pool_in_hbm, pool_in, local_sem.at[2]),
        pltpu.make_async_copy(pool_out_hbm, pool_out, local_sem.at[3]),
        pltpu.make_async_copy(gate_hbm.at[0], gate.at[0], local_sem.at[4]),
        pltpu.make_async_copy(up_hbm.at[0], up.at[0], local_sem.at[5]),
        pltpu.make_async_copy(down_hbm.at[0], down.at[0], local_sem.at[6]),
        pltpu.make_async_copy(exp_gain_hbm, exp_gain, local_sem.at[7]),
        pltpu.make_async_copy(routes_hbm, routes, local_sem.at[8]),
        pltpu.make_async_copy(mix_gain_hbm, mix_gain, local_sem.at[9]),
        pltpu.make_async_copy(pool_map_hbm, pool_map, local_sem.at[10]),
        pltpu.make_async_copy(pool_scale_hbm, pool_scale, local_sem.at[11]),
        pltpu.make_async_copy(group_router_hbm, group_router, local_sem.at[12]),
        pltpu.make_async_copy(expert_router_hbm, expert_router, local_sem.at[13]),
    ]
    for i in (0, 7, 8, 1, 2, 9, 3, 10, 11, 4, 5, 6, 12, 13):
        local[i].start()

    spans = [pl.ds(sum(BACK[:k]), BACK[k]) for k in range(len(BACK))]

    def gate_copy(k):
        return remote(
            gate_hbm.at[0, cols(k)], gate.at[1, cols(k)], ws.at[0, k], wr.at[0, k], ep, mate
        )

    def up_copy(k):
        return remote(up_hbm.at[0, cols(k)], up.at[1, cols(k)], ws.at[1, k], wr.at[1, k], ep, mate)

    def down_copy(k):
        return remote(
            down_hbm.at[0, :, spans[k]],
            down.at[1, :, spans[k]],
            ds.at[k],
            dr.at[k],
            ep,
            mate,
        )

    def y_copy(src, dst, send, recv, k, at, d):
        to = (yc + d) % n
        return remote(src.at[part(to), at], dst.at[part(yc), at], send, recv.at[k], z * n + to, tp)

    def z_copy(src, dst, send, recv, k, at, d):
        to = (z + d) % n
        return remote(src.at[part(to), at], dst.at[part(z), at], send, recv.at[k], to * n + yc, tp)

    def start_all(copy, *args):
        @pl.loop(0, n - 1)
        def _(i):
            copy(*args, n // 2 + (i + 1) // 2 * (1 - 2 * (i % 2))).start()

    others = pl.ds(0, slots - block)

    def recv_all(copy, src, dst, send, recv, k, at):
        remote(src.at[others, at], dst.at[others, at], send, recv.at[k], ep, mate).wait_recv()

    def sent_all(src, send):
        remote(src.at[others], src.at[others], send, zr.at[0], ep, mate).wait_send()

    y_out = (y_copy, ysend, ybuf, ys, yr)
    z_out = (z_copy, zsend, rows.at[0], zs, zr)
    z_early = (z_copy, zsend, ybuf, zs, zr)
    y_late = (y_copy, ysend, yland, ys, yr)
    z_back = (z_copy, zsend2, zbuf2, zs2, zr2)
    y_back = (y_copy, ysend2, ybuf2, ys2, yr2)

    local[0].wait()
    local[7].wait()
    local[8].wait()
    normed[...] = norm_rows(xin[...], exp_gain[...])
    everyone = routes.shape[1]
    named = routes[...].astype(F32)
    here = iota((tokens, everyone), 1) == tp * tokens + iota((tokens, everyone), 0)
    first, second = [
        jnp.sum(jnp.where(here, named[j : j + 1, :], 0.0), axis=1, keepdims=True).astype(jnp.int32)
        for j in range(2)
    ]
    here = iota((everyone, tokens), 0) == tp * tokens + iota((everyone, tokens), 1)
    named = dot(named.astype(BF16), ones_where(here)).astype(jnp.int32)
    lanes = iota((experts, tokens), 0)
    routed = jnp.where((named[0:1, :] == lanes) | (named[1:2, :] == lanes), 1.0, 0.0)
    earlier = ones_where(iota((tokens, tokens), 0) < iota((tokens, tokens), 1))
    rank = (routed * (dot(routed.astype(BF16), earlier) + 1.0)).astype(BF16)

    def slot_of(shape, dim):
        c = iota(shape, dim)
        outer = over(c, n * cap)
        inner = over(c - outer * (n * cap), cap)
        return outer, inner, c - outer * (n * cap) - inner * cap

    def packing(z_major):
        outer, inner, _ = slot_of((slots, experts), 0)
        expert = outer * n + inner if z_major else inner * n + outer
        ranks = dot(ones_where(iota((slots, experts), 1) == expert), rank)
        return ones_where(ranks == (slot_of((slots, tokens), 0)[2] + 1).astype(F32))

    early = pl.ds(0, Z_FIRST * width)
    late = pl.ds(Z_FIRST * width, model - Z_FIRST * width)
    zsend[:, early] = dot(packing(True), normed[:, early]).astype(BF16)
    ysend[:, late] = dot(packing(False), normed[:, late]).astype(BF16)

    local[1].wait()
    local[2].wait()
    local[9].wait()
    total = mix_in.shape[0]
    step = 128

    def pool_rows(b):
        at = pl.multiple_of(b * step, step)
        good = norm_rows(mix_in[pl.ds(at, step), :], mix_gain[...])
        pin[pl.ds(at + step, step), :] = dot(good, pool_in[...]).astype(BF16)

    pool_rows(total // step - 1)
    border_copy = remote(
        pin.at[pl.ds(total + step - RIM, RIM)], border, ms.at[0], mr.at[0], ahead, tp
    )

    with scope("barrier"):
        pl.semaphore_wait(barrier, 2 * (n - 1) + 4)
    border_copy.start()

    gate_copy(0).start()
    up_copy(0).start()
    for k in range(Z_FIRST):
        start_all(*z_early, k, cols(k))
    for k in range(Z_FIRST, Z_FIRST + 3):
        start_all(*y_out, k, cols(k))

    @pl.loop(1, CHUNKS - 1)
    def _(k):
        gate_copy(k).start()
        up_copy(k).start()

    down_copy(0).start()
    gate_copy(CHUNKS - 1).start()
    up_copy(CHUNKS - 1).start()
    for k in range(1, len(BACK)):
        down_copy(k).start()

    ybuf[part(z), early] = zsend[part(z), early]
    ybuf[part(yc), late] = ysend[part(yc), late]

    outer, inner, place = slot_of((slots, slots), 0)
    perm[...] = ones_where(iota((slots, slots), 1) == inner * block + outer * cap + place)

    def to_y(k):
        with scope("wait_z"):
            recv_all(*z_early, k, cols(k))
        ysend[:, cols(k)] = dot(perm[...], ybuf[:, cols(k)]).astype(BF16)
        start_all(*y_late, k, cols(k))
        yland[part(yc), cols(k)] = ysend[part(yc), cols(k)]

    def to_z(k):
        with scope("wait_y"):
            recv_all(*y_out, k, cols(k))
        zsend[:, cols(k)] = dot(perm[...], ybuf[:, cols(k)]).astype(BF16)
        start_all(*z_out, k, cols(k))
        rows[0, part(z), cols(k)] = zsend[part(z), cols(k)]
        part_copy(k, 0).start()

    def part_copy(k, d):
        at = part((z + d) % n)
        return remote(
            rows.at[0, at, cols(k)], rows.at[1, at, cols(k)], rs.at[k], rr.at[k], ep, across
        )

    def row_copy(k):
        return remote(rows.at[0, :, cols(k)], rows.at[1, :, cols(k)], rs.at[k], rr.at[k], ep, across)

    def arrive_late(k):
        with scope("wait_y"):
            recv_all(*y_late, k, cols(k))
        rows[0, :, cols(k)] = dot(perm[...], yland[:, cols(k)]).astype(BF16)
        row_copy(k).start()

    def arrive(k):
        with scope("wait_z"):
            recv_all(*z_out, k, cols(k))

        @pl.loop(1, n)
        def _(d):
            part_copy(k, d).start()


    pl.loop(0, total // step - 1)(pool_rows)
    with scope("wait_border"):
        border_copy.wait_recv()
    pin[pl.ds(0, step - RIM), :] = jnp.zeros((step - RIM, pin.shape[1]), BF16)
    edge = border[...].astype(F32)
    pin[pl.ds(step - RIM, RIM), :] = jnp.where(ep == 0, jnp.zeros_like(edge), edge).astype(BF16)
    window = jnp.left_shift(jnp.int32(2), tp)
    back = iota((step, 2 * step), 0) + step - iota((step, 2 * step), 1)
    band = ones_where((back >= 0) & (back < window))
    local[3].wait()
    local[10].wait()
    local[11].wait()

    @pl.loop(0, total // step)
    def _(b):
        at = pl.multiple_of(b * step, step)
        window_sum = dot(band, pin[pl.ds(at, 2 * step), :])
        position = ep * total + at + iota((step, 1), 0)
        count = jnp.minimum(position + 1, window).astype(F32)
        own = pin[pl.ds(at + step, step), :].astype(F32)
        pooled = (window_sum / count - own).astype(BF16)
        mixed[pl.ds(at, step), :] = (
            dot(pooled, pool_map[0]) * pool_scale[...].astype(F32)[None, :]
        ).astype(BF16)

    quarter = total // 4
    wide = model // PIECES

    def quarter_rows(index):
        return pl.ds(pl.multiple_of(index * quarter, quarter), quarter)

    def piece(j):
        return pl.ds(j * wide, wide)

    def steps(j):
        return (across, mate) if j < ACROSS_FIRST else (mate, across)

    def mix_copy1(j, s):
        return remote(
            mpart.at[quarter_rows(3 - mate if s else steps(j)[0]), piece(j)],
            mrecv1.at[s, :, piece(j)],
            mix1s.at[j, s],
            mix1r.at[j, s],
            ep,
            steps(j)[0],
        )

    def mix_copy2(j):
        return remote(
            msend2.at[:, piece(j)], mrecv2.at[:, piece(j)], mix2s.at[j], mix2r.at[j], ep, steps(j)[1]
        )

    def mix_project(j):
        mpart[:, piece(j)] = dot(mixed[...], pool_out[:, piece(j)]).astype(BF16)
        mix_copy1(j, 0).start()
        mix_copy1(j, 1).start()

    def mix_stage(j):
        with scope("wait_mix1"):
            mix_copy1(j, 0).wait_recv()
            mix_copy1(j, 1).wait_recv()
        msend2[:, piece(j)] = (
            mpart[quarter_rows(steps(j)[1]), piece(j)].astype(F32)
            + mrecv1[1, :, piece(j)].astype(F32)
        ).astype(BF16)
        mix_copy2(j).start()

    def mix_out_copy(j):
        return pltpu.make_async_copy(
            mix_fin.at[:, piece(j)], mix_out.at[:, piece(j)], mix_sem.at[j]
        )

    def mix_finish(j):
        with scope("wait_mix2"):
            mix_copy2(j).wait_recv()
        mix_fin[:, piece(j)] = (
            mpart[quarter_rows(tp), piece(j)].astype(F32)
            + mrecv1[0, :, piece(j)].astype(F32)
            + mrecv2[:, piece(j)].astype(F32)
        ).astype(BF16)
        mix_out_copy(j).start()

    for j in range(ACROSS_FIRST):
        mix_project(j)
    to_z(Z_FIRST)
    to_z(Z_FIRST + 1)
    to_y(0)
    start_all(*y_out, Z_FIRST + 3, cols(Z_FIRST + 3))
    to_z(Z_FIRST + 2)
    for j in range(ACROSS_FIRST, PIECES):
        mix_project(j)
    to_y(1)
    for k in range(Z_FIRST + 4, CHUNKS):
        start_all(*y_out, k, cols(k))
    arrive_late(0)
    to_z(Z_FIRST + 3)
    arrive_late(1)
    arrive(Z_FIRST)
    to_z(Z_FIRST + 4)
    arrive(Z_FIRST + 1)
    to_z(Z_FIRST + 5)

    gsum[...] = jnp.zeros_like(gsum)
    usum[...] = jnp.zeros_like(usum)
    for i in (4, 5, 6, 12, 13):
        local[i].wait()

    def accumulate(r, w, k):
        x = rows[r, :, cols(k)]
        gsum[r, w] += dot(x, gate[w, cols(k), :])
        usum[r, w] += dot(x, up[w, cols(k), :])

    @pl.loop(0, Z_FIRST + 2)
    def _(k):
        accumulate(0, 0, k)

    @pl.loop(Z_FIRST + 2, CHUNKS)
    def _(k):
        arrive(k)
        accumulate(0, 0, k)

    for j in range(ACROSS_FIRST):
        mix_stage(j)

    lanes = iota((tokens, experts), 1)
    routed = jnp.where((first == lanes) | (second == lanes), 1.0, 0.0)
    earlier = ones_where(iota((tokens, tokens), 1) < iota((tokens, tokens), 0))
    rank = (routed * (dot(earlier, routed.astype(BF16)) + 1.0)).astype(BF16)
    outer, inner, _ = slot_of((experts, slots), 1)
    ranks = dot(rank, ones_where(iota((experts, slots), 0) == inner * n + outer))
    outer, inner, place = slot_of((tokens, slots), 1)
    expert = inner * n + outer
    chosen = ranks == (place + 1).astype(F32)
    pick[pl.ds(0, tokens), :] = ones_where(chosen & (first == expert))
    pick[pl.ds(tokens, tokens), :] = ones_where(chosen & (second == expert))
    own_rows = normed[...]
    group_exp = jnp.exp(dot_t(own_rows, group_router[...]))
    group_prob = group_exp / jnp.sum(group_exp, axis=1, keepdims=True)
    expert_exp = jnp.exp(dot_t(own_rows, expert_router[...]))
    groups = group_exp.shape[1]
    ratio = jnp.zeros_like(expert_exp)
    for q in range(groups):
        inside = over(lanes, experts // groups) == q
        within = jnp.sum(jnp.where(inside, expert_exp, 0.0), axis=1, keepdims=True)
        ratio = ratio + jnp.where(inside, group_prob[:, q : q + 1] / within, 0.0)
    prob = expert_exp * ratio
    picked0 = jnp.sum(jnp.where(first == lanes, prob, 0.0), axis=1, keepdims=True)
    picked1 = jnp.sum(jnp.where(second == lanes, prob, 0.0), axis=1, keepdims=True)
    weight0 = picked0 / (picked0 + picked1)
    weight1 = picked1 / (picked0 + picked1)

    def wait_weights(k):
        with scope("wait_w"):
            gate_copy(k).wait_recv()
            up_copy(k).wait_recv()

    def wait_rows(k):
        with scope("wait_r"):
            row_copy(k).wait_recv()

    @pl.loop(0, CHUNKS - 1)
    def _(k):
        wait_weights(k)
        accumulate(0, 1, k)
        wait_rows(k)
        accumulate(1, 0, k)
        accumulate(1, 1, k)

    def activate(r):
        @pl.loop(0, 2)
        def _(w):
            hidden[r, w] = (jax.nn.silu(gsum[r, w]) * usum[r, w]).astype(BF16)

    def partial_copy(k):
        at = spans[k]
        return remote(psend.at[:, at], precv.at[:, at], ps.at[k], pr.at[k], ep, across)

    def project(r, at):
        return dot(hidden[r, 0], down[0, :, at]) + dot(hidden[r, 1], down[1, :, at])

    def down_stage(k):
        at = spans[k]
        with scope("wait_down"):
            down_copy(k).wait_recv()
        psend[:, at] = project(1, at).astype(BF16)
        partial_copy(k).start()
        if k == 0:
            accumulate(0, 1, CHUNKS - 1)
            activate(0)
        pown[:, at] = project(0, at)

    def z_stage(k):
        at = spans[k]
        with scope("wait_part"):
            partial_copy(k).wait_recv()
        zsend2[:, at] = (pown[:, at] + precv[:, at].astype(F32)).astype(BF16)
        start_all(*z_back, k, at)
        zbuf2[part(z), at] = zsend2[part(z), at]

    def y_stage(k):
        at = spans[k]
        with scope("wait_zb"):
            recv_all(*z_back, k, at)
        ysend2[:, at] = dot(perm[...], zbuf2[:, at]).astype(BF16)
        start_all(*y_back, k, at)
        ybuf2[part(yc), at] = ysend2[part(yc), at]

    def exp_copy(k):
        at = spans[k]
        return pltpu.make_async_copy(exp_fin.at[:, at], exp_out.at[:, at], exp_sem.at[k])

    def finish(k):
        at = spans[k]
        with scope("wait_yb"):
            recv_all(*y_back, k, at)
        both = dot(pick[...], ybuf2[:, at])
        exp_fin[:, at] = (weight0 * both[:tokens] + weight1 * both[tokens:]).astype(BF16)
        exp_copy(k).start()

    last = CHUNKS - 1
    wait_rows(last)
    accumulate(1, 0, last)
    wait_weights(last)
    accumulate(1, 1, last)
    activate(1)
    stages = ((down_stage, 0), (z_stage, 2), (y_stage, 4), (finish, 6))
    for turn in range(len(BACK) + 6):
        for stage, later in stages:
            if 0 <= turn - later < len(BACK):
                with scope(stage.__name__):
                    stage(turn - later)
        if 0 <= turn - len(BACK) + 1 < PIECES - ACROSS_FIRST:
            mix_stage(turn - len(BACK) + 1 + ACROSS_FIRST)
        if turn == 1:
            border_copy.wait_send()
            sent_all(ysend, ys)
            sent_all(zsend, zs)

            @pl.loop(0, CHUNKS)
            def _(k):
                gate_copy(k).wait_send()
                up_copy(k).wait_send()
                row_copy(k).wait_send()

        if turn == len(BACK) + 3:
            for j in range(PIECES - 1):
                mix_finish(j)
    mix_finish(PIECES - 1)

    with scope("sent"):
        sent_all(zsend2, zs2)
        sent_all(ysend2, ys2)

        for j in range(PIECES):
            mix_copy1(j, 0).wait_send()
            mix_copy1(j, 1).wait_send()
            mix_copy2(j).wait_send()

        for k in range(len(BACK)):
            down_copy(k).wait_send()
            partial_copy(k).wait_send()
            exp_copy(k).wait()

        for j in range(PIECES):
            mix_out_copy(j).wait()


def write_out(mix_from, exp_from, mix_to, exp_to, mix_held, exp_held, in_sem, out_sem):
    whole = ((mix_from, mix_held, mix_to), (exp_from, exp_held, exp_to))

    def copies(i, h):
        source, held, target = whole[i]
        size = held.shape[0] // 2
        at = pl.ds(h * size, size)
        return (
            pltpu.make_async_copy(source.at[at], held.at[at], in_sem.at[i, h]),
            pltpu.make_async_copy(held.at[at], target.at[at], out_sem.at[i, h]),
        )

    each = [copies(i, h) for i in range(2) for h in range(2)]
    for copy_in, _ in each:
        copy_in.start()
    for copy_in, copy_out in each:
        copy_in.wait()
        copy_out.start()
    for _, copy_out in each:
        copy_out.wait()


def on_device(n, *args):
    (
        mixer_input,
        mixer_gain,
        pool_in,
        pool_map,
        pool_scale,
        pool_out,
        expert_input,
        expert_gain,
        group_router,
        expert_router,
        routes,
        gate_weight,
        up_weight,
        down_weight,
    ) = args
    total, model = mixer_input.shape
    channels = pool_in.shape[1]
    tokens = expert_input.shape[0] // 4
    experts = expert_router.shape[1]
    cap = 4 * tokens // experts
    slots = cap * experts
    hid = gate_weight.shape[2]
    hbm = pl.BlockSpec(memory_space=pl.ANY)
    dma = pltpu.SemaphoreType.DMA
    each, back = dma((CHUNKS,)), dma((len(BACK),))
    sent = pl.pallas_call(
        functools.partial(kernel, n, cap),
        out_shape=(
            jax.ShapeDtypeStruct((total // 4, model), BF16),
            jax.ShapeDtypeStruct((tokens, model), BF16),
        ),
        in_specs=[hbm] * 14,
        out_specs=(hbm, hbm),
        scratch_shapes=[
            pltpu.VMEM((total, model), BF16),
            pltpu.VMEM((model, channels), BF16),
            pltpu.VMEM((channels, model), BF16),
            pltpu.VMEM((total + 128, channels), BF16),
            pltpu.VMEM((RIM, channels), BF16),
            pltpu.VMEM((total, channels), BF16),
            pltpu.VMEM((total, model), BF16),
            pltpu.VMEM((2, total // 4, model), BF16),
            pltpu.VMEM((total // 4, model), BF16),
            pltpu.VMEM((total // 4, model), BF16),
            pltpu.VMEM((tokens, model), BF16),
            pltpu.VMEM((tokens, model), BF16),
            pltpu.VMEM((slots, slots), BF16),
            pltpu.VMEM((2 * tokens, slots), BF16),
            pltpu.VMEM((slots, model), BF16),
            pltpu.VMEM((slots, model), BF16),
            pltpu.VMEM((slots, model), BF16),
            pltpu.VMEM((2, slots, model), BF16),
            pltpu.VMEM((2, model, hid), BF16),
            pltpu.VMEM((2, model, hid), BF16),
            pltpu.VMEM((2, hid, model), BF16),
            pltpu.VMEM((2, 2, slots, hid), F32),
            pltpu.VMEM((2, 2, slots, hid), F32),
            pltpu.VMEM((2, 2, slots, hid), BF16),
            pltpu.VMEM((slots, model), BF16),
            pltpu.VMEM((slots, model), BF16),
            pltpu.VMEM((slots, model), F32),
            pltpu.VMEM((slots, model), BF16),
            pltpu.VMEM((slots, model), BF16),
            pltpu.VMEM((slots, model), BF16),
            pltpu.VMEM((slots, model), BF16),
            dma((14,)),
            dma,
            each,
            dma,
            each,
            dma,
            back,
            dma,
            back,
            each,
            each,
            back,
            back,
            dma((2, CHUNKS)),
            dma((2, CHUNKS)),
            dma((1,)),
            dma((1,)),
            dma((PIECES, 2)),
            dma((PIECES, 2)),
            dma((PIECES,)),
            dma((PIECES,)),
            pltpu.VMEM((slots, Z_FIRST * model // CHUNKS), BF16),
            pltpu.VMEM((tokens, model), BF16),
            pltpu.VMEM((total // 4, model), BF16),
            dma((len(BACK),)),
            dma((PIECES,)),
            back,
            back,
            pltpu.VMEM((model,), BF16),
            pltpu.VMEM((1, channels, channels), BF16),
            pltpu.VMEM((channels,), BF16),
            pltpu.VMEM((model,), BF16),
            pltpu.VMEM((group_router.shape[1], model), BF16),
            pltpu.VMEM((experts, model), BF16),
            pltpu.VMEM((2, 4 * tokens), jnp.int32),
        ],
        compiler_params=pltpu.CompilerParams(
            collective_id=0, has_side_effects=True, vmem_limit_bytes=60 * 1024 * 1024
        ),
    )(
        mixer_input,
        mixer_gain,
        pool_in,
        pool_map,
        pool_scale,
        pool_out,
        expert_input,
        expert_gain,
        group_router.T,
        expert_router.T,
        routes.T,
        gate_weight,
        up_weight,
        down_weight,
    )
    shapes = [(total // 4, model), (tokens, model)]
    return pl.pallas_call(
        write_out,
        out_shape=tuple(jax.ShapeDtypeStruct(shape, BF16) for shape in shapes),
        in_specs=[hbm, hbm],
        out_specs=(hbm, hbm),
        scratch_shapes=[pltpu.VMEM(shape, BF16) for shape in shapes] + [dma((2, 2)), dma((2, 2))],
        cost_estimate=pl.CostEstimate(flops=0, bytes_accessed=4 * 224 * model, transcendentals=0),
    )(*sent)


def solution(mesh):
    n = 1
    while n * n < mesh.shape["ep"]:
        n += 1
    return jax.shard_map(
        functools.partial(on_device, n),
        mesh=mesh,
        in_specs=(
            P("ep", None),
            P(),
            P(None, "tp"),
            P("tp", None, None),
            P("tp"),
            P("tp", None),
            P("ep", None),
            P(),
            P(),
            P(),
            P("ep", None),
            P("ep", None, "tp"),
            P("ep", None, "tp"),
            P("ep", "tp", None),
        ),
        out_specs=(P(("ep", "tp"), None), P(("ep", "tp"), None)),
        check_vma=False,
    )
```

```python
import functools

import jax
import jax.numpy as jnp
from jax import lax
from jax.experimental import pallas as pl
from jax.experimental.pallas import tpu as pltpu
from jax.sharding import PartitionSpec as P

EPS = 1e-06
RIM = 16
CHUNKS = 8
Z_FIRST = 2
PIECES = 4
ACROSS_FIRST = 1
BACK = (128, 128) + (256,) * 6 + (128, 128)
scope = jax.named_scope
MESH = pl.DeviceIdType.MESH
F32 = jnp.float32
BF16 = jnp.bfloat16


def iota(shape, dim):
    return lax.broadcasted_iota(jnp.int32, shape, dim)


def over(value, divisor):
    return (value * (-(-65536 // divisor))) >> 16


def ones_where(mask):
    return jnp.where(mask, 1.0, 0.0).astype(BF16)


def dot(a, b):
    return jnp.dot(a, b, preferred_element_type=F32)


def dot_t(a, b):
    return lax.dot_general(a, b, (((1,), (1,)), ((), ())), preferred_element_type=F32)


def norm_rows(values, gain):
    floats = values.astype(F32)
    scale = lax.rsqrt(jnp.mean(floats * floats, axis=-1, keepdims=True) + EPS)
    return (floats * scale * gain.astype(F32)[None, :]).astype(BF16)


def kernel(
    n,
    cap,
    mix_hbm,
    mix_gain_hbm,
    pool_in_hbm,
    pool_map_hbm,
    pool_scale_hbm,
    pool_out_hbm,
    exp_hbm,
    exp_gain_hbm,
    group_router_hbm,
    expert_router_hbm,
    routes_hbm,
    gate_hbm,
    up_hbm,
    down_hbm,
    mix_out,
    exp_out,
    mix_in,
    pool_in,
    pool_out,
    pin,
    border,
    mixed,
    mpart,
    mrecv1,
    msend2,
    mrecv2,
    xin,
    normed,
    perm,
    pick,
    ysend,
    ybuf,
    zsend,
    rows,
    gate,
    up,
    down,
    gsum,
    usum,
    hidden,
    psend,
    precv,
    pown,
    zsend2,
    zbuf2,
    ysend2,
    ybuf2,
    local_sem,
    ys,
    yr,
    zs,
    zr,
    ys2,
    yr2,
    zs2,
    zr2,
    rs,
    rr,
    ps,
    pr,
    ws,
    wr,
    ms,
    mr,
    mix1s,
    mix1r,
    mix2s,
    mix2r,
    yland,
    exp_fin,
    mix_fin,
    exp_sem,
    mix_sem,
    ds,
    dr,
    mix_gain,
    pool_map,
    pool_scale,
    exp_gain,
    group_router,
    expert_router,
    routes,
):
    ep, tp = lax.axis_index("ep"), lax.axis_index("tp")
    z, yc = ep // n, ep % n
    devices = n * n
    mate = tp + 1 - 2 * (tp % 2)
    across = 3 - tp
    ahead, behind = (ep + 1) % devices, (ep + devices - 1) % devices
    tokens, model = xin.shape
    experts = expert_router.shape[0]
    slots = ysend.shape[0]
    block = slots // n
    width = model // CHUNKS
    hid = gate.shape[2]

    def cols(k):
        return pl.ds(pl.multiple_of(k * width, width), width)

    def part(index):
        return pl.ds(pl.multiple_of(index * block, 16), block)

    def remote(src, dst, send, recv, ep_to, tp_to):
        return pltpu.make_async_remote_copy(
            src_ref=src,
            dst_ref=dst,
            send_sem=send,
            recv_sem=recv,
            device_id={"ep": ep_to, "tp": tp_to},
            device_id_type=MESH,
        )

    barrier = pltpu.get_barrier_semaphore()

    def greet(ep_to, tp_to):
        pl.semaphore_signal(
            barrier, inc=1, device_id={"ep": ep_to, "tp": tp_to}, device_id_type=MESH
        )

    def turned(i):
        return n // 2 + (i + 1) // 2 * (1 - 2 * (i % 2))

    @pl.loop(0, n - 1)
    def _(i):
        greet(((z + turned(i)) % n) * n + yc, tp)

    @pl.loop(0, n - 1)
    def _(i):
        greet(z * n + (yc + turned(i)) % n, tp)

    greet(ep, mate)
    greet(ep, across)
    greet(ahead, tp)
    greet(behind, tp)
    local = [
        pltpu.make_async_copy(
            exp_hbm.at[pl.ds(pl.multiple_of(tp * tokens, 16), tokens)], xin, local_sem.at[0]
        ),
        pltpu.make_async_copy(mix_hbm, mix_in, local_sem.at[1]),
        pltpu.make_async_copy(pool_in_hbm, pool_in, local_sem.at[2]),
        pltpu.make_async_copy(pool_out_hbm, pool_out, local_sem.at[3]),
        pltpu.make_async_copy(gate_hbm.at[0], gate.at[0], local_sem.at[4]),
        pltpu.make_async_copy(up_hbm.at[0], up.at[0], local_sem.at[5]),
        pltpu.make_async_copy(down_hbm.at[0], down.at[0], local_sem.at[6]),
        pltpu.make_async_copy(exp_gain_hbm, exp_gain, local_sem.at[7]),
        pltpu.make_async_copy(routes_hbm, routes, local_sem.at[8]),
        pltpu.make_async_copy(mix_gain_hbm, mix_gain, local_sem.at[9]),
        pltpu.make_async_copy(pool_map_hbm, pool_map, local_sem.at[10]),
        pltpu.make_async_copy(pool_scale_hbm, pool_scale, local_sem.at[11]),
        pltpu.make_async_copy(group_router_hbm, group_router, local_sem.at[12]),
        pltpu.make_async_copy(expert_router_hbm, expert_router, local_sem.at[13]),
    ]
    for i in (0, 7, 8, 1, 2, 9, 3, 10, 11, 4, 5, 6, 12, 13):
        local[i].start()

    spans = [pl.ds(sum(BACK[:k]), BACK[k]) for k in range(len(BACK))]

    def gate_copy(k):
        return remote(
            gate_hbm.at[0, cols(k)], gate.at[1, cols(k)], ws.at[0, k], wr.at[0, k], ep, mate
        )

    def up_copy(k):
        return remote(up_hbm.at[0, cols(k)], up.at[1, cols(k)], ws.at[1, k], wr.at[1, k], ep, mate)

    def down_copy(k):
        return remote(
            down_hbm.at[0, :, spans[k]],
            down.at[1, :, spans[k]],
            ds.at[k],
            dr.at[k],
            ep,
            mate,
        )

    def y_copy(src, dst, send, recv, k, at, d):
        to = (yc + d) % n
        return remote(src.at[part(to), at], dst.at[part(yc), at], send, recv.at[k], z * n + to, tp)

    def z_copy(src, dst, send, recv, k, at, d):
        to = (z + d) % n
        return remote(src.at[part(to), at], dst.at[part(z), at], send, recv.at[k], to * n + yc, tp)

    def start_all(copy, *args):
        @pl.loop(0, n - 1)
        def _(i):
            copy(*args, turned(i)).start()

    others = pl.ds(0, slots - block)

    def recv_all(copy, src, dst, send, recv, k, at):
        remote(src.at[others, at], dst.at[others, at], send, recv.at[k], ep, mate).wait_recv()

    def sent_all(src, send):
        remote(src.at[others], src.at[others], send, zr.at[0], ep, mate).wait_send()

    y_out = (y_copy, ysend, ybuf, ys, yr)
    z_out = (z_copy, zsend, rows.at[0], zs, zr)
    z_early = (z_copy, zsend, ybuf, zs, zr)
    y_late = (y_copy, ysend, yland, ys, yr)
    z_back = (z_copy, zsend2, zbuf2, zs2, zr2)
    y_back = (y_copy, ysend2, ybuf2, ys2, yr2)

    local[0].wait()
    local[7].wait()
    local[8].wait()
    normed[...] = norm_rows(xin[...], exp_gain[...])
    everyone = routes.shape[1]
    named = routes[...].astype(F32)
    here = iota((tokens, everyone), 1) == tp * tokens + iota((tokens, everyone), 0)
    first, second = [
        jnp.sum(jnp.where(here, named[j : j + 1, :], 0.0), axis=1, keepdims=True).astype(jnp.int32)
        for j in range(2)
    ]
    here = iota((everyone, tokens), 0) == tp * tokens + iota((everyone, tokens), 1)
    named = dot(named.astype(BF16), ones_where(here)).astype(jnp.int32)
    lanes = iota((experts, tokens), 0)
    routed = jnp.where((named[0:1, :] == lanes) | (named[1:2, :] == lanes), 1.0, 0.0)
    earlier = ones_where(iota((tokens, tokens), 0) < iota((tokens, tokens), 1))
    rank = (routed * (dot(routed.astype(BF16), earlier) + 1.0)).astype(BF16)

    def slot_of(shape, dim):
        c = iota(shape, dim)
        outer = over(c, n * cap)
        inner = over(c - outer * (n * cap), cap)
        return outer, inner, c - outer * (n * cap) - inner * cap

    def packing(z_major):
        outer, inner, _ = slot_of((slots, experts), 0)
        expert = outer * n + inner if z_major else inner * n + outer
        ranks = dot(ones_where(iota((slots, experts), 1) == expert), rank)
        return ones_where(ranks == (slot_of((slots, tokens), 0)[2] + 1).astype(F32))

    early = pl.ds(0, Z_FIRST * width)
    late = pl.ds(Z_FIRST * width, model - Z_FIRST * width)
    zsend[:, early] = dot(packing(True), normed[:, early]).astype(BF16)
    ysend[:, late] = dot(packing(False), normed[:, late]).astype(BF16)

    local[1].wait()
    local[2].wait()
    local[9].wait()
    total = mix_in.shape[0]
    step = 128

    def pool_rows(b):
        at = pl.multiple_of(b * step, step)
        good = norm_rows(mix_in[pl.ds(at, step), :], mix_gain[...])
        pin[pl.ds(at + step, step), :] = dot(good, pool_in[...]).astype(BF16)

    pool_rows(total // step - 1)
    border_copy = remote(
        pin.at[pl.ds(total + step - RIM, RIM)], border, ms.at[0], mr.at[0], ahead, tp
    )

    with scope("barrier"):
        pl.semaphore_wait(barrier, 2 * (n - 1) + 4)
    border_copy.start()

    gate_copy(0).start()
    up_copy(0).start()
    for k in range(Z_FIRST):
        start_all(*z_early, k, cols(k))
    for k in range(Z_FIRST, Z_FIRST + 3):
        start_all(*y_out, k, cols(k))

    @pl.loop(1, CHUNKS - 1)
    def _(k):
        gate_copy(k).start()
        up_copy(k).start()

    down_copy(0).start()
    gate_copy(CHUNKS - 1).start()
    up_copy(CHUNKS - 1).start()
    for k in range(1, len(BACK)):
        down_copy(k).start()

    ybuf[part(z), early] = zsend[part(z), early]
    ybuf[part(yc), late] = ysend[part(yc), late]

    outer, inner, place = slot_of((slots, slots), 0)
    perm[...] = ones_where(iota((slots, slots), 1) == inner * block + outer * cap + place)

    def to_y(k):
        with scope("wait_z"):
            recv_all(*z_early, k, cols(k))
        ysend[:, cols(k)] = dot(perm[...], ybuf[:, cols(k)]).astype(BF16)
        start_all(*y_late, k, cols(k))
        yland[part(yc), cols(k)] = ysend[part(yc), cols(k)]

    def to_z(k):
        with scope("wait_y"):
            recv_all(*y_out, k, cols(k))
        zsend[:, cols(k)] = dot(perm[...], ybuf[:, cols(k)]).astype(BF16)
        start_all(*z_out, k, cols(k))
        rows[0, part(z), cols(k)] = zsend[part(z), cols(k)]
        part_copy(k, 0).start()

    def part_copy(k, d):
        at = part((z + d) % n)
        return remote(
            rows.at[0, at, cols(k)], rows.at[1, at, cols(k)], rs.at[k], rr.at[k], ep, across
        )

    def row_copy(k):
        return remote(rows.at[0, :, cols(k)], rows.at[1, :, cols(k)], rs.at[k], rr.at[k], ep, across)

    def arrive_late(k):
        with scope("wait_y"):
            recv_all(*y_late, k, cols(k))
        rows[0, :, cols(k)] = dot(perm[...], yland[:, cols(k)]).astype(BF16)
        row_copy(k).start()

    def arrive(k):
        with scope("wait_z"):
            recv_all(*z_out, k, cols(k))

        @pl.loop(1, n)
        def _(d):
            part_copy(k, d).start()


    pl.loop(0, total // step - 1)(pool_rows)
    with scope("wait_border"):
        border_copy.wait_recv()
    pin[pl.ds(0, step - RIM), :] = jnp.zeros((step - RIM, pin.shape[1]), BF16)
    edge = border[...].astype(F32)
    pin[pl.ds(step - RIM, RIM), :] = jnp.where(ep == 0, jnp.zeros_like(edge), edge).astype(BF16)
    window = jnp.left_shift(jnp.int32(2), tp)
    back = iota((step, 2 * step), 0) + step - iota((step, 2 * step), 1)
    band = ones_where((back >= 0) & (back < window))
    local[3].wait()
    local[10].wait()
    local[11].wait()

    @pl.loop(0, total // step)
    def _(b):
        at = pl.multiple_of(b * step, step)
        window_sum = dot(band, pin[pl.ds(at, 2 * step), :])
        position = ep * total + at + iota((step, 1), 0)
        count = jnp.minimum(position + 1, window).astype(F32)
        own = pin[pl.ds(at + step, step), :].astype(F32)
        pooled = (window_sum / count - own).astype(BF16)
        mixed[pl.ds(at, step), :] = (
            dot(pooled, pool_map[0]) * pool_scale[...].astype(F32)[None, :]
        ).astype(BF16)

    quarter = total // 4
    wide = model // PIECES

    def quarter_rows(index):
        return pl.ds(pl.multiple_of(index * quarter, quarter), quarter)

    def piece(j):
        return pl.ds(j * wide, wide)

    def steps(j):
        return (across, mate) if j < ACROSS_FIRST else (mate, across)

    def mix_copy1(j, s):
        return remote(
            mpart.at[quarter_rows(3 - mate if s else steps(j)[0]), piece(j)],
            mrecv1.at[s, :, piece(j)],
            mix1s.at[j, s],
            mix1r.at[j, s],
            ep,
            steps(j)[0],
        )

    def mix_copy2(j):
        return remote(
            msend2.at[:, piece(j)], mrecv2.at[:, piece(j)], mix2s.at[j], mix2r.at[j], ep, steps(j)[1]
        )

    def mix_project(j):
        mpart[:, piece(j)] = dot(mixed[...], pool_out[:, piece(j)]).astype(BF16)
        mix_copy1(j, 0).start()
        mix_copy1(j, 1).start()

    def mix_stage(j):
        with scope("wait_mix1"):
            mix_copy1(j, 0).wait_recv()
            mix_copy1(j, 1).wait_recv()
        msend2[:, piece(j)] = (
            mpart[quarter_rows(steps(j)[1]), piece(j)].astype(F32)
            + mrecv1[1, :, piece(j)].astype(F32)
        ).astype(BF16)
        mix_copy2(j).start()

    def mix_out_copy(j):
        return pltpu.make_async_copy(
            mix_fin.at[:, piece(j)], mix_out.at[:, piece(j)], mix_sem.at[j]
        )

    def mix_finish(j):
        with scope("wait_mix2"):
            mix_copy2(j).wait_recv()
        mix_fin[:, piece(j)] = (
            mpart[quarter_rows(tp), piece(j)].astype(F32)
            + mrecv1[0, :, piece(j)].astype(F32)
            + mrecv2[:, piece(j)].astype(F32)
        ).astype(BF16)
        mix_out_copy(j).start()

    for j in range(ACROSS_FIRST):
        mix_project(j)
    to_z(Z_FIRST)
    to_z(Z_FIRST + 1)
    to_y(0)
    start_all(*y_out, Z_FIRST + 3, cols(Z_FIRST + 3))
    to_z(Z_FIRST + 2)
    for j in range(ACROSS_FIRST, PIECES):
        mix_project(j)
    to_y(1)
    for k in range(Z_FIRST + 4, CHUNKS):
        start_all(*y_out, k, cols(k))
    arrive_late(0)
    to_z(Z_FIRST + 3)
    arrive_late(1)
    arrive(Z_FIRST)
    to_z(Z_FIRST + 4)
    arrive(Z_FIRST + 1)
    to_z(Z_FIRST + 5)

    gsum[...] = jnp.zeros_like(gsum)
    usum[...] = jnp.zeros_like(usum)
    for i in (4, 5, 6, 12, 13):
        local[i].wait()

    def accumulate(r, w, k):
        x = rows[r, :, cols(k)]
        gsum[r, w] += dot(x, gate[w, cols(k), :])
        usum[r, w] += dot(x, up[w, cols(k), :])

    @pl.loop(0, Z_FIRST + 2)
    def _(k):
        accumulate(0, 0, k)

    @pl.loop(Z_FIRST + 2, CHUNKS)
    def _(k):
        arrive(k)
        accumulate(0, 0, k)

    for j in range(ACROSS_FIRST):
        mix_stage(j)

    lanes = iota((tokens, experts), 1)
    routed = jnp.where((first == lanes) | (second == lanes), 1.0, 0.0)
    earlier = ones_where(iota((tokens, tokens), 1) < iota((tokens, tokens), 0))
    rank = (routed * (dot(earlier, routed.astype(BF16)) + 1.0)).astype(BF16)
    outer, inner, _ = slot_of((experts, slots), 1)
    ranks = dot(rank, ones_where(iota((experts, slots), 0) == inner * n + outer))
    outer, inner, place = slot_of((tokens, slots), 1)
    expert = inner * n + outer
    chosen = ranks == (place + 1).astype(F32)
    pick[pl.ds(0, tokens), :] = ones_where(chosen & (first == expert))
    pick[pl.ds(tokens, tokens), :] = ones_where(chosen & (second == expert))
    own_rows = normed[...]
    group_exp = jnp.exp(dot_t(own_rows, group_router[...]))
    group_prob = group_exp / jnp.sum(group_exp, axis=1, keepdims=True)
    expert_exp = jnp.exp(dot_t(own_rows, expert_router[...]))
    groups = group_exp.shape[1]
    ratio = jnp.zeros_like(expert_exp)
    for q in range(groups):
        inside = over(lanes, experts // groups) == q
        within = jnp.sum(jnp.where(inside, expert_exp, 0.0), axis=1, keepdims=True)
        ratio = ratio + jnp.where(inside, group_prob[:, q : q + 1] / within, 0.0)
    prob = expert_exp * ratio
    picked0 = jnp.sum(jnp.where(first == lanes, prob, 0.0), axis=1, keepdims=True)
    picked1 = jnp.sum(jnp.where(second == lanes, prob, 0.0), axis=1, keepdims=True)
    weight0 = picked0 / (picked0 + picked1)
    weight1 = picked1 / (picked0 + picked1)

    def wait_weights(k):
        with scope("wait_w"):
            gate_copy(k).wait_recv()
            up_copy(k).wait_recv()

    def wait_rows(k):
        with scope("wait_r"):
            row_copy(k).wait_recv()

    @pl.loop(0, CHUNKS - 1)
    def _(k):
        wait_weights(k)
        accumulate(0, 1, k)
        wait_rows(k)
        accumulate(1, 0, k)
        accumulate(1, 1, k)

    def activate(r):
        @pl.loop(0, 2)
        def _(w):
            hidden[r, w] = (jax.nn.silu(gsum[r, w]) * usum[r, w]).astype(BF16)

    def partial_copy(k):
        at = spans[k]
        return remote(psend.at[:, at], precv.at[:, at], ps.at[k], pr.at[k, 0], ep, across)


    def block_copy(k, d):
        at, rows_at = spans[k], part((z + d) % n)
        return remote(
            psend.at[rows_at, at],
            precv.at[rows_at, at],
            ps.at[k],
            pr.at[k, d],
            ep,
            across,
        )

    def project(r, at):
        return dot(hidden[r, 0], down[0, :, at]) + dot(hidden[r, 1], down[1, :, at])

    def down_stage(k):
        at = spans[k]
        with scope("wait_down"):
            down_copy(k).wait_recv()
        psend[:, at] = project(1, at).astype(BF16)

        @pl.loop(0, n - 1)
        def _(i):
            block_copy(k, turned(i)).start()

        block_copy(k, 0).start()
        if k == 0:
            accumulate(0, 1, CHUNKS - 1)
            activate(0)
        pown[:, at] = project(0, at)

    def z_stage(k):
        at = spans[k]

        def add(rows_at):
            return (pown[rows_at, at] + precv[rows_at, at].astype(F32)).astype(BF16)

        @pl.loop(0, n - 1)
        def _(i):
            d = turned(i)
            with scope("wait_part"):
                block_copy(k, d).wait_recv()
            rows_at = part((z + d) % n)
            zsend2[rows_at, at] = add(rows_at)
            z_copy(*z_back[1:], k, at, d).start()

        block_copy(k, 0).wait_recv()
        zbuf2[part(z), at] = add(part(z))

    def y_stage(k):
        at = spans[k]
        with scope("wait_zb"):
            recv_all(*z_back, k, at)
        ysend2[:, at] = dot(perm[...], zbuf2[:, at]).astype(BF16)
        start_all(*y_back, k, at)
        ybuf2[part(yc), at] = ysend2[part(yc), at]

    def exp_copy(k):
        at = spans[k]
        return pltpu.make_async_copy(exp_fin.at[:, at], exp_out.at[:, at], exp_sem.at[k])

    def finish(k):
        at = spans[k]
        with scope("wait_yb"):
            recv_all(*y_back, k, at)
        both = dot(pick[...], ybuf2[:, at])
        exp_fin[:, at] = (weight0 * both[:tokens] + weight1 * both[tokens:]).astype(BF16)
        exp_copy(k).start()

    last = CHUNKS - 1
    wait_rows(last)
    accumulate(1, 0, last)
    wait_weights(last)
    accumulate(1, 1, last)
    activate(1)
    stages = ((down_stage, 0), (z_stage, 2), (y_stage, 4), (finish, 6))
    for turn in range(len(BACK) + 6):
        for stage, later in stages:
            if 0 <= turn - later < len(BACK):
                with scope(stage.__name__):
                    stage(turn - later)
        if 0 <= turn - len(BACK) + 1 < PIECES - ACROSS_FIRST:
            mix_stage(turn - len(BACK) + 1 + ACROSS_FIRST)
        if turn == 1:
            border_copy.wait_send()
            sent_all(ysend, ys)
            sent_all(zsend, zs)

            @pl.loop(0, CHUNKS)
            def _(k):
                gate_copy(k).wait_send()
                up_copy(k).wait_send()
                row_copy(k).wait_send()

        if turn == len(BACK) + 3:
            for j in range(PIECES - 1):
                mix_finish(j)
    mix_finish(PIECES - 1)

    with scope("sent"):
        sent_all(zsend2, zs2)
        sent_all(ysend2, ys2)

        for j in range(PIECES):
            mix_copy1(j, 0).wait_send()
            mix_copy1(j, 1).wait_send()
            mix_copy2(j).wait_send()

        for k in range(len(BACK)):
            down_copy(k).wait_send()
            partial_copy(k).wait_send()
            exp_copy(k).wait()

        for j in range(PIECES):
            mix_out_copy(j).wait()


def write_out(mix_from, exp_from, mix_to, exp_to, mix_held, exp_held, in_sem, out_sem):
    whole = ((mix_from, mix_held, mix_to), (exp_from, exp_held, exp_to))

    def copies(i, h):
        source, held, target = whole[i]
        size = held.shape[0] // 2
        at = pl.ds(h * size, size)
        return (
            pltpu.make_async_copy(source.at[at], held.at[at], in_sem.at[i, h]),
            pltpu.make_async_copy(held.at[at], target.at[at], out_sem.at[i, h]),
        )

    each = [copies(i, h) for i in range(2) for h in range(2)]
    for copy_in, _ in each:
        copy_in.start()
    for copy_in, copy_out in each:
        copy_in.wait()
        copy_out.start()
    for _, copy_out in each:
        copy_out.wait()


def on_device(n, *args):
    (
        mixer_input,
        mixer_gain,
        pool_in,
        pool_map,
        pool_scale,
        pool_out,
        expert_input,
        expert_gain,
        group_router,
        expert_router,
        routes,
        gate_weight,
        up_weight,
        down_weight,
    ) = args
    total, model = mixer_input.shape
    channels = pool_in.shape[1]
    tokens = expert_input.shape[0] // 4
    experts = expert_router.shape[1]
    cap = 4 * tokens // experts
    slots = cap * experts
    hid = gate_weight.shape[2]
    hbm = pl.BlockSpec(memory_space=pl.ANY)
    dma = pltpu.SemaphoreType.DMA
    each, back = dma((CHUNKS,)), dma((len(BACK),))
    sent = pl.pallas_call(
        functools.partial(kernel, n, cap),
        out_shape=(
            jax.ShapeDtypeStruct((total // 4, model), BF16),
            jax.ShapeDtypeStruct((tokens, model), BF16),
        ),
        in_specs=[hbm] * 14,
        out_specs=(hbm, hbm),
        scratch_shapes=[
            pltpu.VMEM((total, model), BF16),
            pltpu.VMEM((model, channels), BF16),
            pltpu.VMEM((channels, model), BF16),
            pltpu.VMEM((total + 128, channels), BF16),
            pltpu.VMEM((RIM, channels), BF16),
            pltpu.VMEM((total, channels), BF16),
            pltpu.VMEM((total, model), BF16),
            pltpu.VMEM((2, total // 4, model), BF16),
            pltpu.VMEM((total // 4, model), BF16),
            pltpu.VMEM((total // 4, model), BF16),
            pltpu.VMEM((tokens, model), BF16),
            pltpu.VMEM((tokens, model), BF16),
            pltpu.VMEM((slots, slots), BF16),
            pltpu.VMEM((2 * tokens, slots), BF16),
            pltpu.VMEM((slots, model), BF16),
            pltpu.VMEM((slots, model), BF16),
            pltpu.VMEM((slots, model), BF16),
            pltpu.VMEM((2, slots, model), BF16),
            pltpu.VMEM((2, model, hid), BF16),
            pltpu.VMEM((2, model, hid), BF16),
            pltpu.VMEM((2, hid, model), BF16),
            pltpu.VMEM((2, 2, slots, hid), F32),
            pltpu.VMEM((2, 2, slots, hid), F32),
            pltpu.VMEM((2, 2, slots, hid), BF16),
            pltpu.VMEM((slots, model), BF16),
            pltpu.VMEM((slots, model), BF16),
            pltpu.VMEM((slots, model), F32),
            pltpu.VMEM((slots, model), BF16),
            pltpu.VMEM((slots, model), BF16),
            pltpu.VMEM((slots, model), BF16),
            pltpu.VMEM((slots, model), BF16),
            dma((14,)),
            dma,
            each,
            dma,
            each,
            dma,
            back,
            dma,
            back,
            each,
            each,
            back,
            dma((len(BACK), n)),
            dma((2, CHUNKS)),
            dma((2, CHUNKS)),
            dma((1,)),
            dma((1,)),
            dma((PIECES, 2)),
            dma((PIECES, 2)),
            dma((PIECES,)),
            dma((PIECES,)),
            pltpu.VMEM((slots, Z_FIRST * model // CHUNKS), BF16),
            pltpu.VMEM((tokens, model), BF16),
            pltpu.VMEM((total // 4, model), BF16),
            dma((len(BACK),)),
            dma((PIECES,)),
            back,
            back,
            pltpu.VMEM((model,), BF16),
            pltpu.VMEM((1, channels, channels), BF16),
            pltpu.VMEM((channels,), BF16),
            pltpu.VMEM((model,), BF16),
            pltpu.VMEM((group_router.shape[1], model), BF16),
            pltpu.VMEM((experts, model), BF16),
            pltpu.VMEM((2, 4 * tokens), jnp.int32),
        ],
        compiler_params=pltpu.CompilerParams(
            collective_id=0, has_side_effects=True, vmem_limit_bytes=60 * 1024 * 1024
        ),
    )(
        mixer_input,
        mixer_gain,
        pool_in,
        pool_map,
        pool_scale,
        pool_out,
        expert_input,
        expert_gain,
        group_router.T,
        expert_router.T,
        routes.T,
        gate_weight,
        up_weight,
        down_weight,
    )
    shapes = [(total // 4, model), (tokens, model)]
    return pl.pallas_call(
        write_out,
        out_shape=tuple(jax.ShapeDtypeStruct(shape, BF16) for shape in shapes),
        in_specs=[hbm, hbm],
        out_specs=(hbm, hbm),
        scratch_shapes=[pltpu.VMEM(shape, BF16) for shape in shapes] + [dma((2, 2)), dma((2, 2))],
        cost_estimate=pl.CostEstimate(flops=0, bytes_accessed=4 * 224 * model, transcendentals=0),
    )(*sent)


def solution(mesh):
    n = 1
    while n * n < mesh.shape["ep"]:
        n += 1
    return jax.shard_map(
        functools.partial(on_device, n),
        mesh=mesh,
        in_specs=(
            P("ep", None),
            P(),
            P(None, "tp"),
            P("tp", None, None),
            P("tp"),
            P("tp", None),
            P("ep", None),
            P(),
            P(),
            P(),
            P("ep", None),
            P("ep", None, "tp"),
            P("ep", None, "tp"),
            P("ep", "tp", None),
        ),
        out_specs=(P(("ep", "tp"), None), P(("ep", "tp"), None)),
        check_vma=False,
    )
```

```python
import functools

import jax
import jax.numpy as jnp
from jax import lax
from jax.experimental import pallas as pl
from jax.experimental.pallas import tpu as pltpu
from jax.sharding import PartitionSpec as P

EPS = 1e-06
RIM = 16
CHUNKS = 8
Z_FIRST = 2
PIECES = 4
ACROSS_FIRST = 1
BACK = (128, 128) + (256,) * 6 + (128, 128)
scope = jax.named_scope
MESH = pl.DeviceIdType.MESH
F32 = jnp.float32
BF16 = jnp.bfloat16


def iota(shape, dim):
    return lax.broadcasted_iota(jnp.int32, shape, dim)


def over(value, divisor):
    return (value * (-(-65536 // divisor))) >> 16


def ones_where(mask):
    return jnp.where(mask, 1.0, 0.0).astype(BF16)


def dot(a, b):
    return jnp.dot(a, b, preferred_element_type=F32)


def dot_t(a, b):
    return lax.dot_general(a, b, (((1,), (1,)), ((), ())), preferred_element_type=F32)


def norm_rows(values, gain):
    floats = values.astype(F32)
    scale = lax.rsqrt(jnp.mean(floats * floats, axis=-1, keepdims=True) + EPS)
    return (floats * scale * gain.astype(F32)[None, :]).astype(BF16)


def kernel(
    n,
    cap,
    mix_hbm,
    mix_gain_hbm,
    pool_in_hbm,
    pool_map_hbm,
    pool_scale_hbm,
    pool_out_hbm,
    exp_hbm,
    exp_gain_hbm,
    group_router_hbm,
    expert_router_hbm,
    routes_hbm,
    gate_hbm,
    up_hbm,
    down_hbm,
    mix_out,
    exp_out,
    mix_in,
    pool_in,
    pool_out,
    pin,
    border,
    mixed,
    mpart,
    mrecv1,
    msend2,
    mrecv2,
    xin,
    normed,
    perm,
    pick,
    ysend,
    ybuf,
    zsend,
    rows,
    gate,
    up,
    down,
    gsum,
    usum,
    hidden,
    psend,
    precv,
    pown,
    zsend2,
    zbuf2,
    ysend2,
    ybuf2,
    local_sem,
    ys,
    yr,
    zs,
    zr,
    ys2,
    yr2,
    zs2,
    zr2,
    rs,
    rr,
    ps,
    pr,
    ws,
    wr,
    ms,
    mr,
    mix1s,
    mix1r,
    mix2s,
    mix2r,
    yland,
    exp_fin,
    mix_fin,
    exp_sem,
    mix_sem,
    ds,
    dr,
    mix_gain,
    pool_map,
    pool_scale,
    exp_gain,
    group_router,
    expert_router,
    routes,
):
    ep, tp = lax.axis_index("ep"), lax.axis_index("tp")
    z, yc = ep // n, ep % n
    devices = n * n
    mate = tp + 1 - 2 * (tp % 2)
    across = 3 - tp
    ahead, behind = (ep + 1) % devices, (ep + devices - 1) % devices
    tokens, model = xin.shape
    experts = expert_router.shape[0]
    slots = ysend.shape[0]
    block = slots // n
    width = model // CHUNKS
    hid = gate.shape[2]

    def cols(k):
        return pl.ds(pl.multiple_of(k * width, width), width)

    def part(index):
        return pl.ds(pl.multiple_of(index * block, 16), block)

    def remote(src, dst, send, recv, ep_to, tp_to):
        return pltpu.make_async_remote_copy(
            src_ref=src,
            dst_ref=dst,
            send_sem=send,
            recv_sem=recv,
            device_id={"ep": ep_to, "tp": tp_to},
            device_id_type=MESH,
        )

    barrier = pltpu.get_barrier_semaphore()

    def greet(ep_to, tp_to):
        pl.semaphore_signal(
            barrier, inc=1, device_id={"ep": ep_to, "tp": tp_to}, device_id_type=MESH
        )

    def turned(i):
        return n // 2 + (i + 1) // 2 * (1 - 2 * (i % 2))

    @pl.loop(0, n - 1)
    def _(i):
        greet(((z + turned(i)) % n) * n + yc, tp)

    @pl.loop(0, n - 1)
    def _(i):
        greet(z * n + (yc + turned(i)) % n, tp)

    greet(ep, mate)
    greet(ep, across)
    greet(ahead, tp)
    greet(behind, tp)
    local = [
        pltpu.make_async_copy(
            exp_hbm.at[pl.ds(pl.multiple_of(tp * tokens, 16), tokens)], xin, local_sem.at[0]
        ),
        pltpu.make_async_copy(mix_hbm, mix_in, local_sem.at[1]),
        pltpu.make_async_copy(pool_in_hbm, pool_in, local_sem.at[2]),
        pltpu.make_async_copy(pool_out_hbm, pool_out, local_sem.at[3]),
        pltpu.make_async_copy(gate_hbm.at[0], gate.at[0], local_sem.at[4]),
        pltpu.make_async_copy(up_hbm.at[0], up.at[0], local_sem.at[5]),
        pltpu.make_async_copy(down_hbm.at[0], down.at[0], local_sem.at[6]),
        pltpu.make_async_copy(exp_gain_hbm, exp_gain, local_sem.at[7]),
        pltpu.make_async_copy(routes_hbm, routes, local_sem.at[8]),
        pltpu.make_async_copy(mix_gain_hbm, mix_gain, local_sem.at[9]),
        pltpu.make_async_copy(pool_map_hbm, pool_map, local_sem.at[10]),
        pltpu.make_async_copy(pool_scale_hbm, pool_scale, local_sem.at[11]),
        pltpu.make_async_copy(group_router_hbm, group_router, local_sem.at[12]),
        pltpu.make_async_copy(expert_router_hbm, expert_router, local_sem.at[13]),
    ]
    for i in (0, 7, 8, 1, 2, 9, 3, 10, 11, 4, 5, 6, 12, 13):
        local[i].start()

    spans = [pl.ds(sum(BACK[:k]), BACK[k]) for k in range(len(BACK))]

    def gate_copy(k):
        return remote(
            gate_hbm.at[0, cols(k)], gate.at[1, cols(k)], ws.at[0, k], wr.at[0, k], ep, mate
        )

    def up_copy(k):
        return remote(up_hbm.at[0, cols(k)], up.at[1, cols(k)], ws.at[1, k], wr.at[1, k], ep, mate)

    def down_copy(k):
        return remote(
            down_hbm.at[0, :, spans[k]],
            down.at[1, :, spans[k]],
            ds.at[k],
            dr.at[k],
            ep,
            mate,
        )

    def y_copy(src, dst, send, recv, k, at, d):
        to = (yc + d) % n
        return remote(src.at[part(to), at], dst.at[part(yc), at], send, recv.at[k], z * n + to, tp)

    def z_copy(src, dst, send, recv, k, at, d):
        to = (z + d) % n
        return remote(src.at[part(to), at], dst.at[part(z), at], send, recv.at[k], to * n + yc, tp)

    def start_all(copy, *args):
        @pl.loop(0, n - 1)
        def _(i):
            copy(*args, turned(i)).start()

    others = pl.ds(0, slots - block)

    def recv_all(copy, src, dst, send, recv, k, at):
        remote(src.at[others, at], dst.at[others, at], send, recv.at[k], ep, mate).wait_recv()

    def sent_all(src, send):
        remote(src.at[others], src.at[others], send, zr.at[0], ep, mate).wait_send()

    y_out = (y_copy, ysend, ybuf, ys, yr)
    z_out = (z_copy, zsend, rows.at[0], zs, zr)
    z_early = (z_copy, zsend, ybuf, zs, zr)
    y_late = (y_copy, ysend, yland, ys, yr)
    z_back = (z_copy, zsend2, zbuf2, zs2, zr2)
    y_back = (y_copy, ysend2, ybuf2, ys2, yr2)

    local[0].wait()
    local[7].wait()
    local[8].wait()
    normed[...] = norm_rows(xin[...], exp_gain[...])
    everyone = routes.shape[1]
    named = routes[...].astype(F32)
    here = iota((tokens, everyone), 1) == tp * tokens + iota((tokens, everyone), 0)
    first, second = [
        jnp.sum(jnp.where(here, named[j : j + 1, :], 0.0), axis=1, keepdims=True).astype(jnp.int32)
        for j in range(2)
    ]
    here = iota((everyone, tokens), 0) == tp * tokens + iota((everyone, tokens), 1)
    named = dot(named.astype(BF16), ones_where(here)).astype(jnp.int32)
    lanes = iota((experts, tokens), 0)
    routed = jnp.where((named[0:1, :] == lanes) | (named[1:2, :] == lanes), 1.0, 0.0)
    earlier = ones_where(iota((tokens, tokens), 0) < iota((tokens, tokens), 1))
    rank = (routed * (dot(routed.astype(BF16), earlier) + 1.0)).astype(BF16)

    def slot_of(shape, dim):
        c = iota(shape, dim)
        outer = over(c, n * cap)
        inner = over(c - outer * (n * cap), cap)
        return outer, inner, c - outer * (n * cap) - inner * cap

    def packing(z_major):
        outer, inner, _ = slot_of((slots, experts), 0)
        expert = outer * n + inner if z_major else inner * n + outer
        ranks = dot(ones_where(iota((slots, experts), 1) == expert), rank)
        return ones_where(ranks == (slot_of((slots, tokens), 0)[2] + 1).astype(F32))

    early = pl.ds(0, Z_FIRST * width)
    late = pl.ds(Z_FIRST * width, model - Z_FIRST * width)
    zsend[:, early] = dot(packing(True), normed[:, early]).astype(BF16)
    ysend[:, late] = dot(packing(False), normed[:, late]).astype(BF16)

    local[1].wait()
    local[2].wait()
    local[9].wait()
    total = mix_in.shape[0]
    step = 128

    def pool_rows(b):
        at = pl.multiple_of(b * step, step)
        good = norm_rows(mix_in[pl.ds(at, step), :], mix_gain[...])
        pin[pl.ds(at + step, step), :] = dot(good, pool_in[...]).astype(BF16)

    pool_rows(total // step - 1)
    border_copy = remote(
        pin.at[pl.ds(total + step - RIM, RIM)], border, ms.at[0], mr.at[0], ahead, tp
    )

    with scope("barrier"):
        pl.semaphore_wait(barrier, 2 * (n - 1) + 4)
    border_copy.start()

    gate_copy(0).start()
    up_copy(0).start()
    for k in range(Z_FIRST):
        start_all(*z_early, k, cols(k))
    for k in range(Z_FIRST, Z_FIRST + 3):
        start_all(*y_out, k, cols(k))

    @pl.loop(1, CHUNKS - 1)
    def _(k):
        gate_copy(k).start()
        up_copy(k).start()

    down_copy(0).start()
    gate_copy(CHUNKS - 1).start()
    up_copy(CHUNKS - 1).start()
    for k in range(1, len(BACK)):
        down_copy(k).start()

    ybuf[part(z), early] = zsend[part(z), early]
    ybuf[part(yc), late] = ysend[part(yc), late]

    outer, inner, place = slot_of((slots, slots), 0)
    perm[...] = ones_where(iota((slots, slots), 1) == inner * block + outer * cap + place)

    def to_y(k):
        with scope("wait_z"):
            recv_all(*z_early, k, cols(k))
        ysend[:, cols(k)] = dot(perm[...], ybuf[:, cols(k)]).astype(BF16)
        start_all(*y_late, k, cols(k))
        yland[part(yc), cols(k)] = ysend[part(yc), cols(k)]

    def to_z(k):
        with scope("wait_y"):
            recv_all(*y_out, k, cols(k))
        zsend[:, cols(k)] = dot(perm[...], ybuf[:, cols(k)]).astype(BF16)
        start_all(*z_out, k, cols(k))
        rows[0, part(z), cols(k)] = zsend[part(z), cols(k)]
        part_copy(k, 0).start()

    def part_copy(k, d):
        at = part((z + d) % n)
        return remote(
            rows.at[0, at, cols(k)], rows.at[1, at, cols(k)], rs.at[k], rr.at[k], ep, across
        )

    def row_copy(k):
        return remote(rows.at[0, :, cols(k)], rows.at[1, :, cols(k)], rs.at[k], rr.at[k], ep, across)

    def arrive_late(k):
        with scope("wait_y"):
            recv_all(*y_late, k, cols(k))
        rows[0, :, cols(k)] = dot(perm[...], yland[:, cols(k)]).astype(BF16)
        row_copy(k).start()

    def arrive(k):
        with scope("wait_z"):
            recv_all(*z_out, k, cols(k))

        @pl.loop(1, n)
        def _(d):
            part_copy(k, d).start()


    pl.loop(0, total // step - 1)(pool_rows)
    with scope("wait_border"):
        border_copy.wait_recv()
    pin[pl.ds(0, step - RIM), :] = jnp.zeros((step - RIM, pin.shape[1]), BF16)
    edge = border[...].astype(F32)
    pin[pl.ds(step - RIM, RIM), :] = jnp.where(ep == 0, jnp.zeros_like(edge), edge).astype(BF16)
    window = jnp.left_shift(jnp.int32(2), tp)
    back = iota((step, 2 * step), 0) + step - iota((step, 2 * step), 1)
    band = ones_where((back >= 0) & (back < window))
    local[3].wait()
    local[10].wait()
    local[11].wait()

    @pl.loop(0, total // step)
    def _(b):
        at = pl.multiple_of(b * step, step)
        window_sum = dot(band, pin[pl.ds(at, 2 * step), :])
        position = ep * total + at + iota((step, 1), 0)
        count = jnp.minimum(position + 1, window).astype(F32)
        own = pin[pl.ds(at + step, step), :].astype(F32)
        pooled = (window_sum / count - own).astype(BF16)
        mixed[pl.ds(at, step), :] = (
            dot(pooled, pool_map[0]) * pool_scale[...].astype(F32)[None, :]
        ).astype(BF16)

    quarter = total // 4
    wide = model // PIECES

    def quarter_rows(index):
        return pl.ds(pl.multiple_of(index * quarter, quarter), quarter)

    def piece(j):
        return pl.ds(j * wide, wide)

    def steps(j):
        return (across, mate) if j < ACROSS_FIRST else (mate, across)

    def mix_copy1(j, s):
        return remote(
            mpart.at[quarter_rows(3 - mate if s else steps(j)[0]), piece(j)],
            mrecv1.at[s, :, piece(j)],
            mix1s.at[j, s],
            mix1r.at[j, s],
            ep,
            steps(j)[0],
        )

    def mix_copy2(j):
        return remote(
            msend2.at[:, piece(j)], mrecv2.at[:, piece(j)], mix2s.at[j], mix2r.at[j], ep, steps(j)[1]
        )

    def mix_project(j):
        mpart[:, piece(j)] = dot(mixed[...], pool_out[:, piece(j)]).astype(BF16)
        mix_copy1(j, 0).start()
        mix_copy1(j, 1).start()

    def mix_stage(j):
        with scope("wait_mix1"):
            mix_copy1(j, 0).wait_recv()
            mix_copy1(j, 1).wait_recv()
        msend2[:, piece(j)] = (
            mpart[quarter_rows(steps(j)[1]), piece(j)].astype(F32)
            + mrecv1[1, :, piece(j)].astype(F32)
        ).astype(BF16)
        mix_copy2(j).start()

    def mix_out_copy(j):
        return pltpu.make_async_copy(
            mix_fin.at[:, piece(j)], mix_out.at[:, piece(j)], mix_sem.at[j]
        )

    def mix_finish(j):
        with scope("wait_mix2"):
            mix_copy2(j).wait_recv()
        mix_fin[:, piece(j)] = (
            mpart[quarter_rows(tp), piece(j)].astype(F32)
            + mrecv1[0, :, piece(j)].astype(F32)
            + mrecv2[:, piece(j)].astype(F32)
        ).astype(BF16)
        mix_out_copy(j).start()

    for j in range(ACROSS_FIRST):
        mix_project(j)
    to_z(Z_FIRST)
    to_z(Z_FIRST + 1)
    to_y(0)
    start_all(*y_out, Z_FIRST + 3, cols(Z_FIRST + 3))
    to_z(Z_FIRST + 2)
    for j in range(ACROSS_FIRST, PIECES):
        mix_project(j)
    to_y(1)
    for k in range(Z_FIRST + 4, CHUNKS):
        start_all(*y_out, k, cols(k))
    arrive_late(0)
    to_z(Z_FIRST + 3)
    arrive_late(1)
    arrive(Z_FIRST)
    to_z(Z_FIRST + 4)
    arrive(Z_FIRST + 1)
    to_z(Z_FIRST + 5)

    gsum[...] = jnp.zeros_like(gsum)
    usum[...] = jnp.zeros_like(usum)
    for i in (4, 5, 6, 12, 13):
        local[i].wait()

    def accumulate(r, w, k):
        x = rows[r, :, cols(k)]
        gsum[r, w] += dot(x, gate[w, cols(k), :])
        usum[r, w] += dot(x, up[w, cols(k), :])

    @pl.loop(0, Z_FIRST + 2)
    def _(k):
        accumulate(0, 0, k)

    @pl.loop(Z_FIRST + 2, CHUNKS)
    def _(k):
        arrive(k)
        accumulate(0, 0, k)

    for j in range(ACROSS_FIRST):
        mix_stage(j)

    lanes = iota((tokens, experts), 1)
    routed = jnp.where((first == lanes) | (second == lanes), 1.0, 0.0)
    earlier = ones_where(iota((tokens, tokens), 1) < iota((tokens, tokens), 0))
    rank = (routed * (dot(earlier, routed.astype(BF16)) + 1.0)).astype(BF16)
    outer, inner, _ = slot_of((experts, slots), 1)
    ranks = dot(rank, ones_where(iota((experts, slots), 0) == inner * n + outer))
    outer, inner, place = slot_of((tokens, slots), 1)
    expert = inner * n + outer
    chosen = ranks == (place + 1).astype(F32)
    pick[pl.ds(0, tokens), :] = ones_where(chosen & (first == expert))
    pick[pl.ds(tokens, tokens), :] = ones_where(chosen & (second == expert))
    own_rows = normed[...]
    group_exp = jnp.exp(dot_t(own_rows, group_router[...]))
    group_prob = group_exp / jnp.sum(group_exp, axis=1, keepdims=True)
    expert_exp = jnp.exp(dot_t(own_rows, expert_router[...]))
    groups = group_exp.shape[1]
    ratio = jnp.zeros_like(expert_exp)
    for q in range(groups):
        inside = over(lanes, experts // groups) == q
        within = jnp.sum(jnp.where(inside, expert_exp, 0.0), axis=1, keepdims=True)
        ratio = ratio + jnp.where(inside, group_prob[:, q : q + 1] / within, 0.0)
    prob = expert_exp * ratio
    picked0 = jnp.sum(jnp.where(first == lanes, prob, 0.0), axis=1, keepdims=True)
    picked1 = jnp.sum(jnp.where(second == lanes, prob, 0.0), axis=1, keepdims=True)
    weight0 = picked0 / (picked0 + picked1)
    weight1 = picked1 / (picked0 + picked1)

    def wait_weights(k):
        with scope("wait_w"):
            gate_copy(k).wait_recv()
            up_copy(k).wait_recv()

    def wait_rows(k):
        with scope("wait_r"):
            row_copy(k).wait_recv()

    @pl.loop(0, CHUNKS - 1)
    def _(k):
        wait_weights(k)
        accumulate(0, 1, k)
        wait_rows(k)
        accumulate(1, 0, k)
        accumulate(1, 1, k)

    def activate(r):
        @pl.loop(0, 2)
        def _(w):
            hidden[r, w] = (jax.nn.silu(gsum[r, w]) * usum[r, w]).astype(BF16)

    def partial_copy(k):
        at = spans[k]
        return remote(psend.at[:, at], precv.at[:, at], ps.at[k], pr.at[k, 0], ep, across)


    def block_copy(k, d):
        at, rows_at = spans[k], part((z + d) % n)
        return remote(
            psend.at[rows_at, at],
            precv.at[rows_at, at],
            ps.at[k],
            pr.at[k, d],
            ep,
            across,
        )

    def project(r, at):
        return dot(hidden[r, 0], down[0, :, at]) + dot(hidden[r, 1], down[1, :, at])

    def down_stage(k):
        at = spans[k]
        with scope("wait_down"):
            down_copy(k).wait_recv()
        psend[:, at] = project(1, at).astype(BF16)

        @pl.loop(0, n - 1)
        def _(i):
            block_copy(k, turned(i)).start()

        block_copy(k, 0).start()
        if k == 0:
            accumulate(0, 1, CHUNKS - 1)
            activate(0)
        pown[:, at] = project(0, at)

    def z_stage(k):
        at = spans[k]

        def add(rows_at):
            return (pown[rows_at, at] + precv[rows_at, at].astype(F32)).astype(BF16)

        @pl.loop(0, n - 1)
        def _(i):
            d = turned(i)
            with scope("wait_part"):
                block_copy(k, d).wait_recv()
            rows_at = part((z + d) % n)
            zsend2[rows_at, at] = add(rows_at)
            z_copy(*z_back[1:], k, at, d).start()

        block_copy(k, 0).wait_recv()
        zbuf2[part(z), at] = add(part(z))

    def y_stage(k):
        at = spans[k]
        with scope("wait_zb"):
            recv_all(*z_back, k, at)
        ysend2[:, at] = dot(perm[...], zbuf2[:, at]).astype(BF16)
        start_all(*y_back, k, at)
        ybuf2[part(yc), at] = ysend2[part(yc), at]

    def exp_copy(k):
        at = spans[k]
        return pltpu.make_async_copy(exp_fin.at[:, at], exp_out.at[:, at], exp_sem.at[k])

    def finish(k):
        at = spans[k]
        with scope("wait_yb"):
            recv_all(*y_back, k, at)
        both = dot(pick[...], ybuf2[:, at])
        exp_fin[:, at] = (weight0 * both[:tokens] + weight1 * both[tokens:]).astype(BF16)
        exp_copy(k).start()

    last = CHUNKS - 1
    wait_rows(last)
    accumulate(1, 0, last)
    wait_weights(last)
    accumulate(1, 1, last)
    activate(1)
    stages = ((down_stage, 0), (z_stage, 2), (y_stage, 4), (finish, 6))
    for turn in range(len(BACK) + 6):
        for stage, later in stages:
            if 0 <= turn - later < len(BACK):
                with scope(stage.__name__):
                    stage(turn - later)
        if 0 <= turn - len(BACK) + 1 < PIECES - ACROSS_FIRST:
            mix_stage(turn - len(BACK) + 1 + ACROSS_FIRST)
        if turn == 1:
            border_copy.wait_send()
            sent_all(ysend, ys)
            sent_all(zsend, zs)

            @pl.loop(0, CHUNKS)
            def _(k):
                gate_copy(k).wait_send()
                up_copy(k).wait_send()
                row_copy(k).wait_send()

        if turn == len(BACK) + 3:
            for j in range(PIECES - 1):
                mix_finish(j)
    mix_finish(PIECES - 1)

    with scope("sent"):
        sent_all(zsend2, zs2)
        sent_all(ysend2, ys2)

        for j in range(PIECES):
            mix_copy1(j, 0).wait_send()
            mix_copy1(j, 1).wait_send()
            mix_copy2(j).wait_send()

        for k in range(len(BACK)):
            down_copy(k).wait_send()
            partial_copy(k).wait_send()
            exp_copy(k).wait()

        for j in range(PIECES):
            mix_out_copy(j).wait()


def write_out(mix_from, exp_from, mix_to, exp_to, sem):
    copies = (
        pltpu.make_async_copy(mix_from, mix_to, sem.at[0]),
        pltpu.make_async_copy(exp_from, exp_to, sem.at[1]),
    )
    for copy in copies:
        copy.start()
    for copy in copies:
        copy.wait()


def on_device(n, *args):
    (
        mixer_input,
        mixer_gain,
        pool_in,
        pool_map,
        pool_scale,
        pool_out,
        expert_input,
        expert_gain,
        group_router,
        expert_router,
        routes,
        gate_weight,
        up_weight,
        down_weight,
    ) = args
    total, model = mixer_input.shape
    channels = pool_in.shape[1]
    tokens = expert_input.shape[0] // 4
    experts = expert_router.shape[1]
    cap = 4 * tokens // experts
    slots = cap * experts
    hid = gate_weight.shape[2]
    hbm = pl.BlockSpec(memory_space=pl.ANY)
    dma = pltpu.SemaphoreType.DMA
    each, back = dma((CHUNKS,)), dma((len(BACK),))
    sent = pl.pallas_call(
        functools.partial(kernel, n, cap),
        out_shape=(
            jax.ShapeDtypeStruct((total // 4, model), BF16),
            jax.ShapeDtypeStruct((tokens, model), BF16),
        ),
        in_specs=[hbm] * 14,
        out_specs=(hbm, hbm),
        scratch_shapes=[
            pltpu.VMEM((total, model), BF16),
            pltpu.VMEM((model, channels), BF16),
            pltpu.VMEM((channels, model), BF16),
            pltpu.VMEM((total + 128, channels), BF16),
            pltpu.VMEM((RIM, channels), BF16),
            pltpu.VMEM((total, channels), BF16),
            pltpu.VMEM((total, model), BF16),
            pltpu.VMEM((2, total // 4, model), BF16),
            pltpu.VMEM((total // 4, model), BF16),
            pltpu.VMEM((total // 4, model), BF16),
            pltpu.VMEM((tokens, model), BF16),
            pltpu.VMEM((tokens, model), BF16),
            pltpu.VMEM((slots, slots), BF16),
            pltpu.VMEM((2 * tokens, slots), BF16),
            pltpu.VMEM((slots, model), BF16),
            pltpu.VMEM((slots, model), BF16),
            pltpu.VMEM((slots, model), BF16),
            pltpu.VMEM((2, slots, model), BF16),
            pltpu.VMEM((2, model, hid), BF16),
            pltpu.VMEM((2, model, hid), BF16),
            pltpu.VMEM((2, hid, model), BF16),
            pltpu.VMEM((2, 2, slots, hid), F32),
            pltpu.VMEM((2, 2, slots, hid), F32),
            pltpu.VMEM((2, 2, slots, hid), BF16),
            pltpu.VMEM((slots, model), BF16),
            pltpu.VMEM((slots, model), BF16),
            pltpu.VMEM((slots, model), F32),
            pltpu.VMEM((slots, model), BF16),
            pltpu.VMEM((slots, model), BF16),
            pltpu.VMEM((slots, model), BF16),
            pltpu.VMEM((slots, model), BF16),
            dma((14,)),
            dma,
            each,
            dma,
            each,
            dma,
            back,
            dma,
            back,
            each,
            each,
            back,
            dma((len(BACK), n)),
            dma((2, CHUNKS)),
            dma((2, CHUNKS)),
            dma((1,)),
            dma((1,)),
            dma((PIECES, 2)),
            dma((PIECES, 2)),
            dma((PIECES,)),
            dma((PIECES,)),
            pltpu.VMEM((slots, Z_FIRST * model // CHUNKS), BF16),
            pltpu.VMEM((tokens, model), BF16),
            pltpu.VMEM((total // 4, model), BF16),
            dma((len(BACK),)),
            dma((PIECES,)),
            back,
            back,
            pltpu.VMEM((model,), BF16),
            pltpu.VMEM((1, channels, channels), BF16),
            pltpu.VMEM((channels,), BF16),
            pltpu.VMEM((model,), BF16),
            pltpu.VMEM((group_router.shape[1], model), BF16),
            pltpu.VMEM((experts, model), BF16),
            pltpu.VMEM((2, 4 * tokens), jnp.int32),
        ],
        compiler_params=pltpu.CompilerParams(
            collective_id=0, has_side_effects=True, vmem_limit_bytes=53504 * 1024
        ),
    )(
        *(
            pltpu.with_memory_space_constraint(value, pltpu.HBM)
            for value in (
                mixer_input,
                mixer_gain,
                pool_in,
                pool_map,
                pool_scale,
                pool_out,
                expert_input,
                expert_gain,
                group_router.T,
                expert_router.T,
                routes.T,
                gate_weight,
                up_weight,
                down_weight,
            )
        )
    )
    shapes = [(total // 4, model), (tokens, model)]
    return pl.pallas_call(
        write_out,
        out_shape=tuple(jax.ShapeDtypeStruct(shape, BF16) for shape in shapes),
        in_specs=[hbm, hbm],
        out_specs=(hbm, hbm),
        scratch_shapes=[dma((2,))],
        compiler_params=pltpu.CompilerParams(vmem_limit_bytes=1 << 20),
        cost_estimate=pl.CostEstimate(flops=0, bytes_accessed=4 * 224 * model, transcendentals=0),
    )(*sent)


def solution(mesh):
    n = 1
    while n * n < mesh.shape["ep"]:
        n += 1
    return jax.shard_map(
        functools.partial(on_device, n),
        mesh=mesh,
        in_specs=(
            P("ep", None),
            P(),
            P(None, "tp"),
            P("tp", None, None),
            P("tp"),
            P("tp", None),
            P("ep", None),
            P(),
            P(),
            P(),
            P("ep", None),
            P("ep", None, "tp"),
            P("ep", None, "tp"),
            P("ep", "tp", None),
        ),
        out_specs=(P(("ep", "tp"), None), P(("ep", "tp"), None)),
        check_vma=False,
    )
```

```python
import functools

import jax
import jax.numpy as jnp
from jax import lax
from jax.experimental import pallas as pl
from jax.experimental.pallas import tpu as pltpu
from jax.sharding import PartitionSpec as P

EPS = 1e-06
RIM = 16
CHUNKS = 8
Z_FIRST = 1
PIECES = 8
ACROSS_FIRST = 1
BACK = (128, 128) + (256,) * 6 + (128, 128)
scope = jax.named_scope
MESH = pl.DeviceIdType.MESH
F32 = jnp.float32
BF16 = jnp.bfloat16


def iota(shape, dim):
    return lax.broadcasted_iota(jnp.int32, shape, dim)


def over(value, divisor):
    return (value * (-(-65536 // divisor))) >> 16


def ones_where(mask):
    return jnp.where(mask, 1.0, 0.0).astype(BF16)


def dot(a, b):
    return jnp.dot(a, b, preferred_element_type=F32)


def dot_t(a, b):
    return lax.dot_general(a, b, (((1,), (1,)), ((), ())), preferred_element_type=F32)


def norm_rows(values, gain):
    floats = values.astype(F32)
    scale = lax.rsqrt(jnp.mean(floats * floats, axis=-1, keepdims=True) + EPS)
    return (floats * scale * gain.astype(F32)[None, :]).astype(BF16)


def kernel(
    n,
    cap,
    mix_hbm,
    mix_gain_hbm,
    pool_in_hbm,
    pool_map_hbm,
    pool_scale_hbm,
    pool_out_hbm,
    exp_hbm,
    exp_gain_hbm,
    group_router_hbm,
    expert_router_hbm,
    routes_hbm,
    gate_hbm,
    up_hbm,
    down_hbm,
    mix_out,
    exp_out,
    mix_in,
    pool_in,
    pool_out,
    pin,
    border,
    mixed,
    mpart,
    mrecv1,
    msend2,
    mrecv2,
    xin,
    normed,
    perm,
    pick,
    ysend,
    ybuf,
    zsend,
    rows,
    gate,
    up,
    down,
    gsum,
    usum,
    hidden,
    psend,
    precv,
    pown,
    zsend2,
    zbuf2,
    ysend2,
    ybuf2,
    local_sem,
    ys,
    yr,
    zs,
    zr,
    ys2,
    yr2,
    zs2,
    zr2,
    rs,
    rr,
    ps,
    pr,
    ws,
    wr,
    ms,
    mr,
    mix1s,
    mix1r,
    mix2s,
    mix2r,
    yland,
    exp_fin,
    mix_fin,
    exp_sem,
    mix_sem,
    ds,
    dr,
    mix_gain,
    pool_map,
    pool_scale,
    exp_gain,
    group_router,
    expert_router,
    routes,
):
    ep, tp = lax.axis_index("ep"), lax.axis_index("tp")
    z, yc = ep // n, ep % n
    devices = n * n
    mate = tp + 1 - 2 * (tp % 2)
    across = 3 - tp
    ahead, behind = (ep + 1) % devices, (ep + devices - 1) % devices
    tokens, model = xin.shape
    experts = expert_router.shape[0]
    slots = ysend.shape[0]
    block = slots // n
    width = model // CHUNKS
    hid = gate.shape[2]

    def cols(k):
        return pl.ds(pl.multiple_of(k * width, width), width)

    def part(index):
        return pl.ds(pl.multiple_of(index * block, 16), block)

    def remote(src, dst, send, recv, ep_to, tp_to):
        return pltpu.make_async_remote_copy(
            src_ref=src,
            dst_ref=dst,
            send_sem=send,
            recv_sem=recv,
            device_id={"ep": ep_to, "tp": tp_to},
            device_id_type=MESH,
        )

    barrier = pltpu.get_barrier_semaphore()

    def greet(ep_to, tp_to):
        pl.semaphore_signal(
            barrier, inc=1, device_id={"ep": ep_to, "tp": tp_to}, device_id_type=MESH
        )

    def turned(i):
        return n // 2 + (i + 1) // 2 * (1 - 2 * (i % 2))

    @pl.loop(0, n - 1)
    def _(i):
        greet(((z + turned(i)) % n) * n + yc, tp)

    @pl.loop(0, n - 1)
    def _(i):
        greet(z * n + (yc + turned(i)) % n, tp)

    greet(ep, mate)
    greet(ep, across)
    greet(ahead, tp)
    greet(behind, tp)
    local = [
        pltpu.make_async_copy(
            exp_hbm.at[pl.ds(pl.multiple_of(tp * tokens, 16), tokens)], xin, local_sem.at[0]
        ),
        pltpu.make_async_copy(mix_hbm, mix_in, local_sem.at[1]),
        pltpu.make_async_copy(pool_in_hbm, pool_in, local_sem.at[2]),
        pltpu.make_async_copy(pool_out_hbm, pool_out, local_sem.at[3]),
        pltpu.make_async_copy(gate_hbm.at[0], gate.at[0], local_sem.at[4]),
        pltpu.make_async_copy(up_hbm.at[0], up.at[0], local_sem.at[5]),
        pltpu.make_async_copy(down_hbm.at[0], down.at[0], local_sem.at[6]),
        pltpu.make_async_copy(exp_gain_hbm, exp_gain, local_sem.at[7]),
        pltpu.make_async_copy(routes_hbm, routes, local_sem.at[8]),
        pltpu.make_async_copy(mix_gain_hbm, mix_gain, local_sem.at[9]),
        pltpu.make_async_copy(pool_map_hbm, pool_map, local_sem.at[10]),
        pltpu.make_async_copy(pool_scale_hbm, pool_scale, local_sem.at[11]),
        pltpu.make_async_copy(group_router_hbm, group_router, local_sem.at[12]),
        pltpu.make_async_copy(expert_router_hbm, expert_router, local_sem.at[13]),
    ]
    for i in (0, 7, 8, 1, 2, 9, 3, 10, 11, 4, 5, 6, 12, 13):
        local[i].start()

    spans = [pl.ds(sum(BACK[:k]), BACK[k]) for k in range(len(BACK))]

    def gate_copy(k):
        return remote(
            gate_hbm.at[0, cols(k)], gate.at[1, cols(k)], ws.at[0, k], wr.at[0, k], ep, mate
        )

    def up_copy(k):
        return remote(up_hbm.at[0, cols(k)], up.at[1, cols(k)], ws.at[1, k], wr.at[1, k], ep, mate)

    def down_copy(k):
        return remote(
            down_hbm.at[0, :, spans[k]],
            down.at[1, :, spans[k]],
            ds.at[k],
            dr.at[k],
            ep,
            mate,
        )

    def y_copy(src, dst, send, recv, k, at, d):
        to = (yc + d) % n
        return remote(src.at[part(to), at], dst.at[part(yc), at], send, recv.at[k], z * n + to, tp)

    def z_copy(src, dst, send, recv, k, at, d):
        to = (z + d) % n
        return remote(src.at[part(to), at], dst.at[part(z), at], send, recv.at[k], to * n + yc, tp)

    def start_all(copy, *args):
        @pl.loop(0, n - 1)
        def _(i):
            copy(*args, turned(i)).start()

    others = pl.ds(0, slots - block)

    def recv_all(copy, src, dst, send, recv, k, at):
        remote(src.at[others, at], dst.at[others, at], send, recv.at[k], ep, mate).wait_recv()

    def sent_all(src, send):
        remote(src.at[others], src.at[others], send, zr.at[0], ep, mate).wait_send()

    y_out = (y_copy, ysend, ybuf, ys, yr)
    z_out = (z_copy, zsend, rows.at[0], zs, zr)
    z_early = (z_copy, zsend, ybuf, zs, zr)
    y_late = (y_copy, ysend, yland, ys, yr)
    z_back = (z_copy, zsend2, zbuf2, zs2, zr2)
    y_back = (y_copy, ysend2, ybuf2, ys2, yr2)

    local[0].wait()
    local[7].wait()
    local[8].wait()
    normed[...] = norm_rows(xin[...], exp_gain[...])
    everyone = routes.shape[1]
    named = routes[...].astype(F32)
    here = iota((tokens, everyone), 1) == tp * tokens + iota((tokens, everyone), 0)
    first, second = [
        jnp.sum(jnp.where(here, named[j : j + 1, :], 0.0), axis=1, keepdims=True).astype(jnp.int32)
        for j in range(2)
    ]
    here = iota((everyone, tokens), 0) == tp * tokens + iota((everyone, tokens), 1)
    named = dot(named.astype(BF16), ones_where(here)).astype(jnp.int32)
    lanes = iota((experts, tokens), 0)
    routed = jnp.where((named[0:1, :] == lanes) | (named[1:2, :] == lanes), 1.0, 0.0)
    earlier = ones_where(iota((tokens, tokens), 0) < iota((tokens, tokens), 1))
    rank = (routed * (dot(routed.astype(BF16), earlier) + 1.0)).astype(BF16)

    def slot_of(shape, dim):
        c = iota(shape, dim)
        outer = over(c, n * cap)
        inner = over(c - outer * (n * cap), cap)
        return outer, inner, c - outer * (n * cap) - inner * cap

    def packing(z_major):
        outer, inner, _ = slot_of((slots, experts), 0)
        expert = outer * n + inner if z_major else inner * n + outer
        ranks = dot(ones_where(iota((slots, experts), 1) == expert), rank)
        return ones_where(ranks == (slot_of((slots, tokens), 0)[2] + 1).astype(F32))

    early = pl.ds(0, Z_FIRST * width)
    late = pl.ds(Z_FIRST * width, model - Z_FIRST * width)
    zsend[:, early] = dot(packing(True), normed[:, early]).astype(BF16)
    ysend[:, late] = dot(packing(False), normed[:, late]).astype(BF16)

    local[1].wait()
    local[2].wait()
    local[9].wait()
    total = mix_in.shape[0]
    step = 128

    def pool_rows(b):
        at = pl.multiple_of(b * step, step)
        good = norm_rows(mix_in[pl.ds(at, step), :], mix_gain[...])
        pin[pl.ds(at + step, step), :] = dot(good, pool_in[...]).astype(BF16)

    pool_rows(total // step - 1)
    border_copy = remote(
        pin.at[pl.ds(total + step - RIM, RIM)], border, ms.at[0], mr.at[0], ahead, tp
    )

    with scope("barrier"):
        pl.semaphore_wait(barrier, 2 * (n - 1) + 4)
    border_copy.start()

    gate_copy(0).start()
    up_copy(0).start()
    for k in range(Z_FIRST):
        start_all(*z_early, k, cols(k))
    for k in range(Z_FIRST, Z_FIRST + 3):
        start_all(*y_out, k, cols(k))

    @pl.loop(1, CHUNKS - 1)
    def _(k):
        gate_copy(k).start()
        up_copy(k).start()

    down_copy(0).start()
    gate_copy(CHUNKS - 1).start()
    up_copy(CHUNKS - 1).start()
    for k in range(1, len(BACK)):
        down_copy(k).start()

    ybuf[part(z), early] = zsend[part(z), early]
    ybuf[part(yc), late] = ysend[part(yc), late]

    outer, inner, place = slot_of((slots, slots), 0)
    perm[...] = ones_where(iota((slots, slots), 1) == inner * block + outer * cap + place)

    def to_y(k):
        with scope("wait_z"):
            recv_all(*z_early, k, cols(k))
        ysend[:, cols(k)] = dot(perm[...], ybuf[:, cols(k)]).astype(BF16)
        start_all(*y_late, k, cols(k))
        yland[part(yc), cols(k)] = ysend[part(yc), cols(k)]

    def to_z(k):
        with scope("wait_y"):
            recv_all(*y_out, k, cols(k))
        zsend[:, cols(k)] = dot(perm[...], ybuf[:, cols(k)]).astype(BF16)
        start_all(*z_out, k, cols(k))
        rows[0, part(z), cols(k)] = zsend[part(z), cols(k)]
        part_copy(k, 0).start()

    def part_copy(k, d):
        at = part((z + d) % n)
        return remote(
            rows.at[0, at, cols(k)], rows.at[1, at, cols(k)], rs.at[k], rr.at[k], ep, across
        )

    def row_copy(k):
        return remote(rows.at[0, :, cols(k)], rows.at[1, :, cols(k)], rs.at[k], rr.at[k], ep, across)

    def arrive_late(k):
        with scope("wait_y"):
            recv_all(*y_late, k, cols(k))
        rows[0, :, cols(k)] = dot(perm[...], yland[:, cols(k)]).astype(BF16)
        row_copy(k).start()

    def arrive(k):
        with scope("wait_z"):
            recv_all(*z_out, k, cols(k))

        @pl.loop(1, n)
        def _(d):
            part_copy(k, d).start()


    pl.loop(0, total // step - 1)(pool_rows)
    with scope("wait_border"):
        border_copy.wait_recv()
    pin[pl.ds(0, step - RIM), :] = jnp.zeros((step - RIM, pin.shape[1]), BF16)
    edge = border[...].astype(F32)
    pin[pl.ds(step - RIM, RIM), :] = jnp.where(ep == 0, jnp.zeros_like(edge), edge).astype(BF16)
    window = jnp.left_shift(jnp.int32(2), tp)
    back = iota((step, 2 * step), 0) + step - iota((step, 2 * step), 1)
    band = ones_where((back >= 0) & (back < window))
    local[3].wait()
    local[10].wait()
    local[11].wait()

    @pl.loop(0, total // step)
    def _(b):
        at = pl.multiple_of(b * step, step)
        window_sum = dot(band, pin[pl.ds(at, 2 * step), :])
        position = ep * total + at + iota((step, 1), 0)
        count = jnp.minimum(position + 1, window).astype(F32)
        own = pin[pl.ds(at + step, step), :].astype(F32)
        pooled = (window_sum / count - own).astype(BF16)
        mixed[pl.ds(at, step), :] = (
            dot(pooled, pool_map[0]) * pool_scale[...].astype(F32)[None, :]
        ).astype(BF16)

    quarter = total // 4
    wide = model // PIECES

    def quarter_rows(index):
        return pl.ds(pl.multiple_of(index * quarter, quarter), quarter)

    def piece(j):
        return pl.ds(j * wide, wide)

    def steps(j):
        return (across, mate) if j < ACROSS_FIRST else (mate, across)

    def mix_copy1(j, s):
        return remote(
            mpart.at[quarter_rows(3 - mate if s else steps(j)[0]), piece(j)],
            mrecv1.at[s, :, piece(j)],
            mix1s.at[j, s],
            mix1r.at[j, s],
            ep,
            steps(j)[0],
        )

    def mix_copy2(j):
        return remote(
            msend2.at[:, piece(j)], mrecv2.at[:, piece(j)], mix2s.at[j], mix2r.at[j], ep, steps(j)[1]
        )

    def mix_project(j):
        mpart[:, piece(j)] = dot(mixed[...], pool_out[:, piece(j)]).astype(BF16)
        mix_copy1(j, 0).start()
        mix_copy1(j, 1).start()

    def mix_stage(j):
        with scope("wait_mix1"):
            mix_copy1(j, 0).wait_recv()
            mix_copy1(j, 1).wait_recv()
        msend2[:, piece(j)] = (
            mpart[quarter_rows(steps(j)[1]), piece(j)].astype(F32)
            + mrecv1[1, :, piece(j)].astype(F32)
        ).astype(BF16)
        mix_copy2(j).start()

    def mix_out_copy(j):
        return pltpu.make_async_copy(
            mix_fin.at[:, piece(j)], mix_out.at[:, piece(j)], mix_sem.at[j]
        )

    def mix_finish(j):
        with scope("wait_mix2"):
            mix_copy2(j).wait_recv()
        mix_fin[:, piece(j)] = (
            mpart[quarter_rows(tp), piece(j)].astype(F32)
            + mrecv1[0, :, piece(j)].astype(F32)
            + mrecv2[:, piece(j)].astype(F32)
        ).astype(BF16)
        mix_out_copy(j).start()

    for j in range(ACROSS_FIRST):
        mix_project(j)
    to_z(1)
    to_z(2)
    to_y(0)
    start_all(*y_out, 4, cols(4))
    to_z(3)
    for j in range(ACROSS_FIRST, PIECES):
        mix_project(j)
    arrive_late(0)
    for k in range(5, CHUNKS):
        start_all(*y_out, k, cols(k))
    arrive(1)
    to_z(4)
    arrive(2)
    to_z(5)
    arrive(3)
    to_z(6)
    to_z(7)

    gsum[...] = jnp.zeros_like(gsum)
    usum[...] = jnp.zeros_like(usum)
    for i in (4, 5, 6, 12, 13):
        local[i].wait()

    def accumulate(r, w, k):
        x = rows[r, :, cols(k)]
        gsum[r, w] += dot(x, gate[w, cols(k), :])
        usum[r, w] += dot(x, up[w, cols(k), :])

    @pl.loop(0, 4)
    def _(k):
        accumulate(0, 0, k)

    @pl.loop(4, CHUNKS)
    def _(k):
        arrive(k)
        accumulate(0, 0, k)

    for j in range(ACROSS_FIRST):
        mix_stage(j)

    lanes = iota((tokens, experts), 1)
    routed = jnp.where((first == lanes) | (second == lanes), 1.0, 0.0)
    earlier = ones_where(iota((tokens, tokens), 1) < iota((tokens, tokens), 0))
    rank = (routed * (dot(earlier, routed.astype(BF16)) + 1.0)).astype(BF16)
    outer, inner, _ = slot_of((experts, slots), 1)
    ranks = dot(rank, ones_where(iota((experts, slots), 0) == inner * n + outer))
    outer, inner, place = slot_of((tokens, slots), 1)
    expert = inner * n + outer
    chosen = ranks == (place + 1).astype(F32)
    pick[pl.ds(0, tokens), :] = ones_where(chosen & (first == expert))
    pick[pl.ds(tokens, tokens), :] = ones_where(chosen & (second == expert))
    own_rows = normed[...]
    group_exp = jnp.exp(dot_t(own_rows, group_router[...]))
    group_prob = group_exp / jnp.sum(group_exp, axis=1, keepdims=True)
    expert_exp = jnp.exp(dot_t(own_rows, expert_router[...]))
    groups = group_exp.shape[1]
    ratio = jnp.zeros_like(expert_exp)
    for q in range(groups):
        inside = over(lanes, experts // groups) == q
        within = jnp.sum(jnp.where(inside, expert_exp, 0.0), axis=1, keepdims=True)
        ratio = ratio + jnp.where(inside, group_prob[:, q : q + 1] / within, 0.0)
    prob = expert_exp * ratio
    picked0 = jnp.sum(jnp.where(first == lanes, prob, 0.0), axis=1, keepdims=True)
    picked1 = jnp.sum(jnp.where(second == lanes, prob, 0.0), axis=1, keepdims=True)
    weight0 = picked0 / (picked0 + picked1)
    weight1 = picked1 / (picked0 + picked1)

    def wait_weights(k):
        with scope("wait_w"):
            gate_copy(k).wait_recv()
            up_copy(k).wait_recv()

    def wait_rows(k):
        with scope("wait_r"):
            row_copy(k).wait_recv()

    @pl.loop(0, CHUNKS - 1)
    def _(k):
        wait_weights(k)
        accumulate(0, 1, k)
        wait_rows(k)
        accumulate(1, 0, k)
        accumulate(1, 1, k)

    def activate(r):
        @pl.loop(0, 2)
        def _(w):
            hidden[r, w] = (jax.nn.silu(gsum[r, w]) * usum[r, w]).astype(BF16)

    def partial_copy(k):
        at = spans[k]
        return remote(psend.at[:, at], precv.at[:, at], ps.at[k], pr.at[k, 0], ep, across)


    def block_copy(k, d):
        at, rows_at = spans[k], part((z + d) % n)
        return remote(
            psend.at[rows_at, at],
            precv.at[rows_at, at],
            ps.at[k],
            pr.at[k, d],
            ep,
            across,
        )

    def project(r, at):
        return dot(hidden[r, 0], down[0, :, at]) + dot(hidden[r, 1], down[1, :, at])

    def down_stage(k):
        at = spans[k]
        with scope("wait_down"):
            down_copy(k).wait_recv()
        psend[:, at] = project(1, at).astype(BF16)

        @pl.loop(0, n - 1)
        def _(i):
            block_copy(k, turned(i)).start()

        block_copy(k, 0).start()
        if k == 0:
            accumulate(0, 1, CHUNKS - 1)
            activate(0)
        pown[:, at] = project(0, at)

    def z_stage(k):
        at = spans[k]

        def add(rows_at):
            return (pown[rows_at, at] + precv[rows_at, at].astype(F32)).astype(BF16)

        @pl.loop(0, n - 1)
        def _(i):
            d = turned(i)
            with scope("wait_part"):
                block_copy(k, d).wait_recv()
            rows_at = part((z + d) % n)
            zsend2[rows_at, at] = add(rows_at)
            z_copy(*z_back[1:], k, at, d).start()

        block_copy(k, 0).wait_recv()
        zbuf2[part(z), at] = add(part(z))

    def y_stage(k):
        at = spans[k]
        with scope("wait_zb"):
            recv_all(*z_back, k, at)
        ysend2[:, at] = dot(perm[...], zbuf2[:, at]).astype(BF16)
        start_all(*y_back, k, at)
        ybuf2[part(yc), at] = ysend2[part(yc), at]

    def exp_copy(k):
        at = spans[k]
        return pltpu.make_async_copy(exp_fin.at[:, at], exp_out.at[:, at], exp_sem.at[k])

    def finish(k):
        at = spans[k]
        with scope("wait_yb"):
            recv_all(*y_back, k, at)
        both = dot(pick[...], ybuf2[:, at])
        exp_fin[:, at] = (weight0 * both[:tokens] + weight1 * both[tokens:]).astype(BF16)
        exp_copy(k).start()

    last = CHUNKS - 1
    wait_rows(last)
    accumulate(1, 0, last)
    wait_weights(last)
    accumulate(1, 1, last)
    activate(1)
    stages = ((down_stage, 0), (z_stage, 2), (y_stage, 4), (finish, 6))
    for turn in range(len(BACK) + 6):
        for stage, later in stages:
            if 0 <= turn - later < len(BACK):
                with scope(stage.__name__):
                    stage(turn - later)
        if turn >= len(BACK) - 1:
            staged = ACROSS_FIRST + 2 * (turn - len(BACK) + 1)
            for j in range(staged, min(staged + 2, PIECES)):
                mix_stage(j)
        if turn == 1:
            border_copy.wait_send()
            sent_all(ysend, ys)
            sent_all(zsend, zs)

            @pl.loop(0, CHUNKS)
            def _(k):
                gate_copy(k).wait_send()
                up_copy(k).wait_send()
                row_copy(k).wait_send()

        if turn == len(BACK) + 3:
            for j in range(PIECES // 2):
                mix_finish(j)
    for j in range(PIECES // 2, PIECES):
        mix_finish(j)

    with scope("sent"):
        sent_all(zsend2, zs2)
        sent_all(ysend2, ys2)

        for j in range(PIECES):
            mix_copy1(j, 0).wait_send()
            mix_copy1(j, 1).wait_send()
            mix_copy2(j).wait_send()

        for k in range(len(BACK)):
            down_copy(k).wait_send()
            partial_copy(k).wait_send()
            exp_copy(k).wait()

        for j in range(PIECES):
            mix_out_copy(j).wait()


def write_out(mix_from, exp_from, mix_to, exp_to, sem):
    copies = (
        pltpu.make_async_copy(mix_from, mix_to, sem.at[0]),
        pltpu.make_async_copy(exp_from, exp_to, sem.at[1]),
    )
    for copy in copies:
        copy.start()
    for copy in copies:
        copy.wait()


def on_device(n, *args):
    (
        mixer_input,
        mixer_gain,
        pool_in,
        pool_map,
        pool_scale,
        pool_out,
        expert_input,
        expert_gain,
        group_router,
        expert_router,
        routes,
        gate_weight,
        up_weight,
        down_weight,
    ) = args
    total, model = mixer_input.shape
    channels = pool_in.shape[1]
    tokens = expert_input.shape[0] // 4
    experts = expert_router.shape[1]
    cap = 4 * tokens // experts
    slots = cap * experts
    hid = gate_weight.shape[2]
    hbm = pl.BlockSpec(memory_space=pl.ANY)
    dma = pltpu.SemaphoreType.DMA
    each, back = dma((CHUNKS,)), dma((len(BACK),))
    sent = pl.pallas_call(
        functools.partial(kernel, n, cap),
        out_shape=(
            jax.ShapeDtypeStruct((total // 4, model), BF16),
            jax.ShapeDtypeStruct((tokens, model), BF16),
        ),
        in_specs=[hbm] * 14,
        out_specs=(hbm, hbm),
        scratch_shapes=[
            pltpu.VMEM((total, model), BF16),
            pltpu.VMEM((model, channels), BF16),
            pltpu.VMEM((channels, model), BF16),
            pltpu.VMEM((total + 128, channels), BF16),
            pltpu.VMEM((RIM, channels), BF16),
            pltpu.VMEM((total, channels), BF16),
            pltpu.VMEM((total, model), BF16),
            pltpu.VMEM((2, total // 4, model), BF16),
            pltpu.VMEM((total // 4, model), BF16),
            pltpu.VMEM((total // 4, model), BF16),
            pltpu.VMEM((tokens, model), BF16),
            pltpu.VMEM((tokens, model), BF16),
            pltpu.VMEM((slots, slots), BF16),
            pltpu.VMEM((2 * tokens, slots), BF16),
            pltpu.VMEM((slots, model), BF16),
            pltpu.VMEM((slots, model), BF16),
            pltpu.VMEM((slots, model), BF16),
            pltpu.VMEM((2, slots, model), BF16),
            pltpu.VMEM((2, model, hid), BF16),
            pltpu.VMEM((2, model, hid), BF16),
            pltpu.VMEM((2, hid, model), BF16),
            pltpu.VMEM((2, 2, slots, hid), F32),
            pltpu.VMEM((2, 2, slots, hid), F32),
            pltpu.VMEM((2, 2, slots, hid), BF16),
            pltpu.VMEM((slots, model), BF16),
            pltpu.VMEM((slots, model), BF16),
            pltpu.VMEM((slots, model), F32),
            pltpu.VMEM((slots, model), BF16),
            pltpu.VMEM((slots, model), BF16),
            pltpu.VMEM((slots, model), BF16),
            pltpu.VMEM((slots, model), BF16),
            dma((14,)),
            dma,
            each,
            dma,
            each,
            dma,
            back,
            dma,
            back,
            each,
            each,
            back,
            dma((len(BACK), n)),
            dma((2, CHUNKS)),
            dma((2, CHUNKS)),
            dma((1,)),
            dma((1,)),
            dma((PIECES, 2)),
            dma((PIECES, 2)),
            dma((PIECES,)),
            dma((PIECES,)),
            pltpu.VMEM((slots, Z_FIRST * model // CHUNKS), BF16),
            pltpu.VMEM((tokens, model), BF16),
            pltpu.VMEM((total // 4, model), BF16),
            dma((len(BACK),)),
            dma((PIECES,)),
            back,
            back,
            pltpu.VMEM((model,), BF16),
            pltpu.VMEM((1, channels, channels), BF16),
            pltpu.VMEM((channels,), BF16),
            pltpu.VMEM((model,), BF16),
            pltpu.VMEM((group_router.shape[1], model), BF16),
            pltpu.VMEM((experts, model), BF16),
            pltpu.VMEM((2, 4 * tokens), jnp.int32),
        ],
        compiler_params=pltpu.CompilerParams(
            collective_id=0, has_side_effects=True, vmem_limit_bytes=53504 * 1024
        ),
    )(
        *(
            pltpu.with_memory_space_constraint(value, pltpu.HBM)
            for value in (
                mixer_input,
                mixer_gain,
                pool_in,
                pool_map,
                pool_scale,
                pool_out,
                expert_input,
                expert_gain,
                group_router.T,
                expert_router.T,
                routes.T,
                gate_weight,
                up_weight,
                down_weight,
            )
        )
    )
    shapes = [(total // 4, model), (tokens, model)]
    return pl.pallas_call(
        write_out,
        out_shape=tuple(jax.ShapeDtypeStruct(shape, BF16) for shape in shapes),
        in_specs=[hbm, hbm],
        out_specs=(hbm, hbm),
        scratch_shapes=[dma((2,))],
        compiler_params=pltpu.CompilerParams(vmem_limit_bytes=1 << 20),
        cost_estimate=pl.CostEstimate(flops=0, bytes_accessed=4 * 224 * model, transcendentals=0),
    )(*sent)


def solution(mesh):
    n = 1
    while n * n < mesh.shape["ep"]:
        n += 1
    return jax.shard_map(
        functools.partial(on_device, n),
        mesh=mesh,
        in_specs=(
            P("ep", None),
            P(),
            P(None, "tp"),
            P("tp", None, None),
            P("tp"),
            P("tp", None),
            P("ep", None),
            P(),
            P(),
            P(),
            P("ep", None),
            P("ep", None, "tp"),
            P("ep", None, "tp"),
            P("ep", "tp", None),
        ),
        out_specs=(P(("ep", "tp"), None), P(("ep", "tp"), None)),
        check_vma=False,
    )
```
